32 devices in a mesh: sp: 16 (over z, y, x), tp: 2 (over core).
Axes of the slice: x: 2, y: 2, z: 4, core: 2. Of those that a mesh axis runs over, the one named last changes fastest.
Arguments:
- resid: bfloat16 [3072, 2048], P('sp'), may hold values from -6 to 6
- query: bfloat16 [3072, 2048], P('sp', 'tp'), may hold values from -6 to 6
- key: bfloat16 [3072, 1024], P('sp', 'tp'), may hold values from -6 to 6
- value: bfloat16 [3072, 1024], P('sp', 'tp'), may hold values from -6 to 6
- q_gain: float32 [128], replicated, may hold values from 0.3 to 5, as said below
- k_gain: float32 [128], replicated, may hold values from 0.3 to 5, as said below
- out_weight: bfloat16 [2048, 2048], P('tp'), may hold values from -0.125 to 0.125
- norm_gain: float32 [2048], replicated, may hold values from 0.1 to 1.9
- gate_weight: bfloat16 [2048, 5632], P('sp', 'tp'), may hold values from -0.125 to 0.125
- up_weight: bfloat16 [2048, 5632], P('sp', 'tp'), may hold values from -0.125 to 0.125
- down_weight: bfloat16 [5632, 2048], P('tp', 'sp'), may hold values from -0.078125 to 0.078125
Outputs:
- mixed: bfloat16 [3072, 2048], P(('sp', 'tp'))
The draws below stay inside these ranges and needn't reach their ends.
Inputs may be any that keep to these rules, and one draw needn't show every extreme that they name: `q_gain`: positive gains. `k_gain`: positive gains.
All inputs are finite; a program needn't handle non-finite values.
Results may differ from the reference program's by a relative error of at most 0.012.
The reference program's roundings to bfloat16 on the way count: a program that leaves them out, or rounds other values in their place, can miss the bound.
Values may be sent and summed in bfloat16 or wider, within the bound.
A program may use at most 128 MiB of HBM per device.

```python
import jax
import jax.numpy as jnp
from jax import lax

D = 2048
HEADS = 16
KV_HEADS = 8
HEAD_DIM = 128
FF = 5632
GRID_W = 64
TOK_DEV = 192
TOKENS = 3072
N_TP = 2


def paired_draw(key):
    base = jax.random.fold_in(key, 11)
    key_rows = jnp.clip(jax.random.normal(jax.random.fold_in(base, 1), (TOKENS, KV_HEADS * HEAD_DIM), jnp.float32), -6.0, 6.0)
    query_rows = jnp.clip(jax.random.normal(jax.random.fold_in(base, 2), (TOKENS, HEADS * HEAD_DIM), jnp.float32), -6.0, 6.0)
    return (query_rows, key_rows)


def draw_query(key, part):
    return paired_draw(key)[0].astype(jnp.bfloat16)


def draw_key(key, part):
    return paired_draw(key)[1].astype(jnp.bfloat16)


def gain_draw(key, salt):
    base = jax.random.fold_in(key, salt)
    return jnp.exp(jax.random.uniform(base, (HEAD_DIM,), jnp.float32, jnp.log(0.6), jnp.log(3.0)))


def draw_q_gain(key, part):
    return gain_draw(key, 21)


def draw_k_gain(key, part):
    return gain_draw(key, 22)


def level_of(key, shape, shards, low, high):
    level, own = 1.0, jax.random.fold_in(key, 6)
    for position, shards_of in shards:
        draws = jnp.exp(jax.random.uniform(jax.random.fold_in(own, position), (shards_of,), jnp.float32, low / len(shards), high / len(shards)))
        level = level * jnp.repeat(draws, shape[position] // shards_of).reshape([-1 if axis == position else 1 for axis in range(len(shape))])
    return level


def normal_values(own_key, extent, deviation, reach, shards=(), kind=jnp.bfloat16):
    entries = deviation * jax.random.normal(own_key, extent, jnp.float32)
    if shards:
        entries = entries * level_of(own_key, extent, shards, -0.22, 0.18)
    return jnp.clip(entries, -reach, reach).astype(kind)


def setup_inputs(seed: int = 0) -> dict:
    splits = jax.random.split(jax.random.key(seed), 12)
    return {
        "resid": normal_values(splits[0], (TOKENS, D), 1.0, 6.0, ((0, 16),)),
        "query": draw_query(jax.random.fold_in(splits[11], 71), 0),
        "key": draw_key(jax.random.fold_in(splits[11], 71), 0),
        "value": normal_values(splits[3], (TOKENS, KV_HEADS * HEAD_DIM), 1.0, 6.0, ((0, 16), (1, 2))),
        "q_gain": draw_q_gain(jax.random.fold_in(splits[11], 71), 0),
        "k_gain": draw_k_gain(jax.random.fold_in(splits[11], 71), 0),
        "out_weight": normal_values(splits[6], (HEADS * HEAD_DIM, D), (HEADS * HEAD_DIM) ** -0.5, 0.125, ((0, 2),)),
        "norm_gain": jnp.clip(1.0 + 0.18 * jax.random.normal(splits[7], (D,), jnp.float32), 0.1, 1.9),
        "gate_weight": normal_values(splits[8], (D, FF), D ** -0.5, 0.125, ((0, 16), (1, 2))),
        "up_weight": normal_values(splits[9], (D, FF), D ** -0.5, 0.125, ((0, 16), (1, 2))),
        "down_weight": normal_values(splits[10], (FF, D), FF ** -0.5, 0.078125, ((0, 2), (1, 16))),
    }


EPSILON = 1e-06

def rounded(values):
    return lax.optimization_barrier(values.astype(jnp.bfloat16)).astype(jnp.float32)

def rotate(values, positions):
    dim_size = values.shape[-1]
    half_dim = dim_size // 2
    quarter = half_dim // 2
    inverse = 10000.0 ** (-jnp.arange(quarter, dtype=jnp.float32) / quarter)
    outputs = []
    for axis_pos, coords in enumerate((positions // GRID_W, positions % GRID_W)):
        angles = coords.astype(jnp.float32)[:, None] * inverse[None, :]
        cosine = jnp.cos(angles)[:, None, :]
        sine = jnp.sin(angles)[:, None, :]
        section = values[..., axis_pos * half_dim:(axis_pos + 1) * half_dim]
        first_half = section[..., :quarter]
        second_half = section[..., quarter:]
        outputs += [first_half * cosine - second_half * sine, second_half * cosine + first_half * sine]
    return jnp.concatenate(outputs, axis=-1)

def prepare(projected, gain, positions):
    values = projected.astype(jnp.float32)
    normed = values * lax.rsqrt(lax.optimization_barrier(jnp.mean(values * values, axis=-1, keepdims=True)) + EPSILON) * gain
    return rotate(normed, positions).astype(jnp.bfloat16)

def normalize(stream, gain):
    values = stream.astype(jnp.float32)
    return (values * lax.rsqrt(lax.optimization_barrier(jnp.mean(values * values, axis=-1, keepdims=True)) + EPSILON) * gain).astype(jnp.bfloat16)

def reference(resid, query, key, value, q_gain, k_gain, out_weight, norm_gain, gate_weight, up_weight, down_weight):
    positions = jnp.arange(TOKENS, dtype=jnp.int32)
    q_rot = prepare(query.reshape(TOKENS, HEADS, HEAD_DIM), q_gain, positions)
    k_rot = prepare(key.reshape(TOKENS, KV_HEADS, HEAD_DIM), k_gain, positions)
    key_float = k_rot.astype(jnp.float32)
    val_float = value.reshape(TOKENS, KV_HEADS, HEAD_DIM).astype(jnp.float32)
    group_size = HEADS // KV_HEADS
    query_blocks = q_rot.reshape(TOKENS // TOK_DEV, TOK_DEV, KV_HEADS, group_size, HEAD_DIM)

    def one_block(block):
        scores = jnp.einsum('qkgd,skd->kgqs', block.astype(jnp.float32), key_float) * HEAD_DIM ** (-0.5)
        maxima = lax.optimization_barrier(jnp.max(scores, axis=-1, keepdims=True))
        weights = jnp.exp(scores - maxima)
        totals = lax.optimization_barrier(jnp.sum(weights, axis=-1))
        summed = jnp.einsum('kgqs,skd->kgqd', rounded(weights), val_float)
        output = summed / totals[..., None]
        return jnp.transpose(output, (2, 0, 1, 3)).reshape(TOK_DEV, HEADS * HEAD_DIM).astype(jnp.bfloat16)
    attn = lax.map(one_block, query_blocks).reshape(TOKENS, HEADS * HEAD_DIM)
    head_width = HEADS * HEAD_DIM // N_TP
    proj = jnp.zeros((TOKENS, D), jnp.float32)
    for index in range(N_TP):
        part_rows = slice(index * head_width, (index + 1) * head_width)
        proj = proj + rounded(jnp.dot(attn[:, part_rows], out_weight[part_rows], preferred_element_type=jnp.float32))
    stream = (resid.astype(jnp.float32) + proj).astype(jnp.bfloat16)
    normed = normalize(stream, norm_gain)
    gate = jnp.dot(normed, gate_weight, preferred_element_type=jnp.float32)
    up_part = jnp.dot(normed, up_weight, preferred_element_type=jnp.float32)
    hidden = (jax.nn.silu(gate) * up_part).astype(jnp.bfloat16)
    unit_width = FF // N_TP
    down = jnp.zeros((TOKENS, D), jnp.float32)
    for index in range(N_TP):
        part_rows = slice(index * unit_width, (index + 1) * unit_width)
        down = down + rounded(jnp.dot(hidden[:, part_rows], down_weight[part_rows], preferred_element_type=jnp.float32))
    return (stream.astype(jnp.float32) + 0.5 * down).astype(jnp.bfloat16)
```

```python
import jax
import jax.numpy as jnp
from jax import lax
from jax.sharding import PartitionSpec as P

GRID_W = 64


EPSILON = 1e-06


def rotate(values, positions):
    dim_size = values.shape[-1]
    half_dim = dim_size // 2
    quarter = half_dim // 2
    inverse = 10000.0 ** (-jnp.arange(quarter, dtype=jnp.float32) / quarter)
    outputs = []
    for axis_pos, coords in enumerate((positions // GRID_W, positions % GRID_W)):
        angles = coords.astype(jnp.float32)[:, None] * inverse[None, :]
        cosine = jnp.cos(angles)[:, None, :]
        sine = jnp.sin(angles)[:, None, :]
        section = values[..., axis_pos * half_dim : (axis_pos + 1) * half_dim]
        first_half = section[..., :quarter]
        second_half = section[..., quarter:]
        outputs += [
            first_half * cosine - second_half * sine,
            second_half * cosine + first_half * sine,
        ]
    return jnp.concatenate(outputs, axis=-1)


def prepare(projected, gain, positions):
    values = projected.astype(jnp.float32)
    normed = values * lax.rsqrt(jnp.mean(values * values, axis=-1, keepdims=True) + EPSILON) * gain
    return rotate(normed, positions).astype(jnp.bfloat16)


def normalize(stream, gain):
    values = stream.astype(jnp.float32)
    return (
        values * lax.rsqrt(jnp.mean(values * values, axis=-1, keepdims=True) + EPSILON) * gain
    ).astype(jnp.bfloat16)


def whole_body(
    resid,
    query,
    key,
    value,
    q_gain,
    k_gain,
    out_weight,
    norm_gain,
    gate_weight,
    up_weight,
    down_weight,
):
    rows_here = query.shape[0]
    head_dim = q_gain.shape[0]
    heads_here = query.shape[1] // head_dim
    kv_here = key.shape[1] // head_dim
    group_size = heads_here // kv_here
    score_scale = head_dim ** (-0.5)
    positions = lax.axis_index("sp") * rows_here + jnp.arange(rows_here, dtype=jnp.int32)
    q_rot = prepare(query.reshape(rows_here, heads_here, head_dim), q_gain, positions)
    k_rot = prepare(key.reshape(rows_here, kv_here, head_dim), k_gain, positions)
    val_rows = value.reshape(rows_here, kv_here, head_dim)
    grouped = q_rot.reshape(rows_here, kv_here, group_size, head_dim)

    def key_block(carry, block):
        maxima, totals, accum = carry
        block_keys, block_vals = block
        scores = (
            jnp.einsum("qkgd,skd->kgqs", grouped, block_keys, preferred_element_type=jnp.float32)
            * score_scale
        )
        new_max = jnp.maximum(maxima, jnp.max(scores, axis=-1))
        shrink = jnp.exp(maxima - new_max)
        weights = jnp.exp(scores - new_max[..., None])
        totals = totals * shrink + jnp.sum(weights, axis=-1)
        accum = accum * shrink[..., None] + jnp.einsum(
            "kgqs,skd->kgqd",
            weights.astype(jnp.bfloat16),
            block_vals,
            preferred_element_type=jnp.float32,
        )
        return ((new_max, totals, accum), None)

    start_max = jnp.full((kv_here, group_size, rows_here), -1e30, jnp.float32)
    start_total = jnp.zeros((kv_here, group_size, rows_here), jnp.float32)
    start_accum = jnp.zeros((kv_here, group_size, rows_here, head_dim), jnp.float32)
    carry = (start_max, start_total, start_accum)
    key_part = lax.all_gather(k_rot, "sp", axis=0, tiled=True)
    val_part = lax.all_gather(val_rows, "sp", axis=0, tiled=True)
    length = key_part.shape[0]
    factor = 4
    span = rows_here * factor
    turns = length // span
    key_blocks = key_part.reshape(turns, span, kv_here, head_dim)
    val_blocks = val_part.reshape(turns, span, kv_here, head_dim)
    carry, _ = lax.scan(key_block, carry, (key_blocks, val_blocks))
    maxima, totals, accum = carry
    attn = (
        jnp.transpose(accum / totals[..., None], (2, 0, 1, 3))
        .reshape(rows_here, heads_here * head_dim)
        .astype(jnp.bfloat16)
    )
    share = rows_here // lax.axis_size("tp")
    my_first = lax.axis_index("tp") * share
    proj = lax.psum_scatter(
        jnp.dot(attn, out_weight, preferred_element_type=jnp.float32).astype(jnp.bfloat16),
        "tp",
        scatter_dimension=0,
        tiled=True,
    ).astype(jnp.float32)
    my_resid = lax.dynamic_slice_in_dim(resid, my_first, share, 0)
    my_stream = (my_resid.astype(jnp.float32) + proj).astype(jnp.bfloat16)
    mixer_rows = lax.all_gather(normalize(my_stream, norm_gain), "tp", axis=0, tiled=True)

    def add_rows(shard_rows):
        return jnp.dot(mixer_rows, shard_rows, preferred_element_type=jnp.float32)

    gate = add_rows(lax.all_gather(gate_weight, "sp", axis=0, tiled=True))
    up_part = add_rows(lax.all_gather(up_weight, "sp", axis=0, tiled=True))
    hidden = (jax.nn.silu(gate) * up_part).astype(jnp.bfloat16)
    down_whole = lax.all_gather(down_weight, "sp", axis=1, tiled=True)
    down = lax.psum_scatter(
        jnp.dot(hidden, down_whole, preferred_element_type=jnp.float32).astype(jnp.bfloat16),
        "tp",
        scatter_dimension=0,
        tiled=True,
    ).astype(jnp.float32)
    return (my_stream.astype(jnp.float32) + 0.5 * down).astype(jnp.bfloat16)


SPLIT = 4


def fits(n_sp, kv_here, hidden_here):
    return n_sp % SPLIT == 0 and kv_here % SPLIT == 0 and hidden_here % (64 * SPLIT) == 0


def groups_of(n_sp):
    ranks = n_sp // SPLIT
    tokens = [[part * ranks + rank for part in range(SPLIT)] for rank in range(ranks)]
    hidden = [[part * ranks + rank for rank in range(ranks)] for part in range(SPLIT)]
    return tokens, hidden


def body(
    resid,
    query,
    key,
    value,
    q_gain,
    k_gain,
    out_weight,
    norm_gain,
    gate_weight,
    up_weight,
    down_weight,
):
    rows = query.shape[0]
    head_dim = q_gain.shape[0]
    heads_here = query.shape[1] // head_dim
    kv_here = key.shape[1] // head_dim
    n_sp = lax.axis_size("sp")
    if not fits(n_sp, kv_here, gate_weight.shape[1]):
        return whole_body(
            resid, query, key, value, q_gain, k_gain, out_weight, norm_gain, gate_weight, up_weight, down_weight
        )
    tok_groups, hid_groups = groups_of(n_sp)
    ranks = n_sp // SPLIT
    group_size = heads_here // kv_here
    kv_part = kv_here // SPLIT

    def swap(array):
        return lax.all_to_all(array, "sp", 0, 0, axis_index_groups=tok_groups, tiled=True)

    def spread(array, axis):
        return lax.all_gather(array, "sp", axis=axis, axis_index_groups=hid_groups, tiled=True)

    positions = lax.axis_index("sp") * rows + jnp.arange(rows, dtype=jnp.int32)
    q_rot = prepare(query.reshape(rows, heads_here, head_dim), q_gain, positions)
    k_rot = prepare(key.reshape(rows, kv_here, head_dim), k_gain, positions)
    cut = lambda a: a.reshape(a.shape[0], SPLIT, -1).transpose(1, 0, 2).reshape(SPLIT * a.shape[0], -1)
    k_rot, val = cut(k_rot), cut(value)
    pair = swap(jnp.concatenate([k_rot, val], axis=1))
    pair = spread(pair, 0)
    q_mine = swap(cut(q_rot))
    width = kv_part * head_dim
    keys = pair[:, :width].reshape(-1, kv_part, head_dim)
    vals = pair[:, width:].reshape(-1, kv_part, head_dim)
    grouped = q_mine.reshape(SPLIT * rows, kv_part, group_size, head_dim)
    gate_up = spread(swap(jnp.concatenate([cut(gate_weight), cut(up_weight)], axis=1)), 0)
    depth = gate_weight.shape[0]
    gate_up = gate_up.reshape(ranks, SPLIT, depth, -1).transpose(1, 0, 2, 3).reshape(n_sp * depth, -1)
    down_w = swap(down_weight)
    part = down_weight.shape[0] // SPLIT
    down_w = down_w.reshape(SPLIT, part, -1)
    down_w = lax.all_gather(down_w, "sp", axis=1, axis_index_groups=hid_groups)
    down_w = jnp.transpose(down_w, (2, 0, 1, 3)).reshape(part, -1)
    scores = jnp.einsum("qkgd,skd->kgqs", grouped, keys, preferred_element_type=jnp.float32) * head_dim ** (-0.5)
    weights = jnp.exp(scores - jnp.max(scores, axis=-1, keepdims=True))
    totals = jnp.sum(weights, axis=-1)
    accum = jnp.einsum("kgqs,skd->kgqd", weights.astype(jnp.bfloat16), vals, preferred_element_type=jnp.float32)
    attn = jnp.transpose(accum / totals[..., None], (2, 0, 1, 3)).astype(jnp.bfloat16).reshape(SPLIT * rows, -1)
    attn = swap(attn).reshape(SPLIT, rows, -1).transpose(1, 0, 2).reshape(rows, -1)
    return finish(attn, resid, out_weight, norm_gain, gate_up, down_w, tok_groups)


def finish(attn, resid, out_weight, norm_gain, gate_up, down_w, tok_groups):
    rows = resid.shape[0]
    n_tp = lax.axis_size("tp")
    share = rows // n_tp
    my_first = lax.axis_index("tp") * share
    proj = lax.psum_scatter(
        jnp.dot(attn, out_weight, preferred_element_type=jnp.float32).astype(jnp.bfloat16),
        "tp",
        scatter_dimension=0,
        tiled=True,
    ).astype(jnp.float32)
    my_resid = lax.dynamic_slice_in_dim(resid, my_first, share, 0)
    my_stream = (my_resid.astype(jnp.float32) + proj).astype(jnp.bfloat16)
    normed = normalize(my_stream, norm_gain)
    normed = lax.all_gather(normed, "sp", axis=0, axis_index_groups=tok_groups, tiled=False)
    normed = lax.all_gather(normed, "tp", axis=0, tiled=False)
    normed = normed.reshape(n_tp * SPLIT * share, -1)
    both = jnp.dot(normed, gate_up, preferred_element_type=jnp.float32)
    gate, up_part = jnp.split(both, 2, axis=1)
    hidden = (jax.nn.silu(gate) * up_part).astype(jnp.bfloat16)
    down = jnp.dot(hidden, down_w, preferred_element_type=jnp.float32).astype(jnp.bfloat16)
    down = lax.psum_scatter(down, "tp", scatter_dimension=0, tiled=True)
    down = lax.all_to_all(
        down.reshape(SPLIT, share, -1), "sp", 0, 0, axis_index_groups=tok_groups, tiled=True
    )
    down = jnp.sum(down.astype(jnp.float32), axis=0)
    return (my_stream.astype(jnp.float32) + 0.5 * down).astype(jnp.bfloat16)


def solution(mesh):
    placed = (
        P("sp", None),
        P("sp", "tp"),
        P("sp", "tp"),
        P("sp", "tp"),
        P(),
        P(),
        P("tp", None),
        P(),
        P("sp", "tp"),
        P("sp", "tp"),
        P("tp", "sp"),
    )
    return jax.shard_map(
        body, mesh=mesh, in_specs=placed, out_specs=P(("sp", "tp"), None), check_vma=False
    )
```

```python
import functools
import math

import jax
import jax.numpy as jnp
from jax import lax
from jax.experimental import pallas as pl
from jax.experimental.pallas import tpu as pltpu
from jax.sharding import PartitionSpec as P

GRID_W = 64


EPSILON = 1e-06


def rotate(values, positions):
    dim_size = values.shape[-1]
    half_dim = dim_size // 2
    quarter = half_dim // 2
    inverse = 10000.0 ** (-jnp.arange(quarter, dtype=jnp.float32) / quarter)
    outputs = []
    for axis_pos, coords in enumerate((positions // GRID_W, positions % GRID_W)):
        angles = coords.astype(jnp.float32)[:, None] * inverse[None, :]
        cosine = jnp.cos(angles)[:, None, :]
        sine = jnp.sin(angles)[:, None, :]
        section = values[..., axis_pos * half_dim : (axis_pos + 1) * half_dim]
        first_half = section[..., :quarter]
        second_half = section[..., quarter:]
        outputs += [
            first_half * cosine - second_half * sine,
            second_half * cosine + first_half * sine,
        ]
    return jnp.concatenate(outputs, axis=-1)


def prepare(projected, gain, positions):
    values = projected.astype(jnp.float32)
    normed = values * lax.rsqrt(jnp.mean(values * values, axis=-1, keepdims=True) + EPSILON) * gain
    return rotate(normed, positions).astype(jnp.bfloat16)


def normalize(stream, gain):
    values = stream.astype(jnp.float32)
    return (
        values * lax.rsqrt(jnp.mean(values * values, axis=-1, keepdims=True) + EPSILON) * gain
    ).astype(jnp.bfloat16)


def whole_body(
    resid,
    query,
    key,
    value,
    q_gain,
    k_gain,
    out_weight,
    norm_gain,
    gate_weight,
    up_weight,
    down_weight,
):
    rows_here = query.shape[0]
    head_dim = q_gain.shape[0]
    heads_here = query.shape[1] // head_dim
    kv_here = key.shape[1] // head_dim
    group_size = heads_here // kv_here
    score_scale = head_dim ** (-0.5)
    positions = lax.axis_index("sp") * rows_here + jnp.arange(rows_here, dtype=jnp.int32)
    q_rot = prepare(query.reshape(rows_here, heads_here, head_dim), q_gain, positions)
    k_rot = prepare(key.reshape(rows_here, kv_here, head_dim), k_gain, positions)
    val_rows = value.reshape(rows_here, kv_here, head_dim)
    grouped = q_rot.reshape(rows_here, kv_here, group_size, head_dim)

    def key_block(carry, block):
        maxima, totals, accum = carry
        block_keys, block_vals = block
        scores = (
            jnp.einsum("qkgd,skd->kgqs", grouped, block_keys, preferred_element_type=jnp.float32)
            * score_scale
        )
        new_max = jnp.maximum(maxima, jnp.max(scores, axis=-1))
        shrink = jnp.exp(maxima - new_max)
        weights = jnp.exp(scores - new_max[..., None])
        totals = totals * shrink + jnp.sum(weights, axis=-1)
        accum = accum * shrink[..., None] + jnp.einsum(
            "kgqs,skd->kgqd",
            weights.astype(jnp.bfloat16),
            block_vals,
            preferred_element_type=jnp.float32,
        )
        return ((new_max, totals, accum), None)

    start_max = jnp.full((kv_here, group_size, rows_here), -1e30, jnp.float32)
    start_total = jnp.zeros((kv_here, group_size, rows_here), jnp.float32)
    start_accum = jnp.zeros((kv_here, group_size, rows_here, head_dim), jnp.float32)
    carry = (start_max, start_total, start_accum)
    key_part = lax.all_gather(k_rot, "sp", axis=0, tiled=True)
    val_part = lax.all_gather(val_rows, "sp", axis=0, tiled=True)
    length = key_part.shape[0]
    factor = 4
    span = rows_here * factor
    turns = length // span
    key_blocks = key_part.reshape(turns, span, kv_here, head_dim)
    val_blocks = val_part.reshape(turns, span, kv_here, head_dim)
    carry, _ = lax.scan(key_block, carry, (key_blocks, val_blocks))
    maxima, totals, accum = carry
    attn = (
        jnp.transpose(accum / totals[..., None], (2, 0, 1, 3))
        .reshape(rows_here, heads_here * head_dim)
        .astype(jnp.bfloat16)
    )
    share = rows_here // lax.axis_size("tp")
    my_first = lax.axis_index("tp") * share
    proj = lax.psum_scatter(
        jnp.dot(attn, out_weight, preferred_element_type=jnp.float32).astype(jnp.bfloat16),
        "tp",
        scatter_dimension=0,
        tiled=True,
    ).astype(jnp.float32)
    my_resid = lax.dynamic_slice_in_dim(resid, my_first, share, 0)
    my_stream = (my_resid.astype(jnp.float32) + proj).astype(jnp.bfloat16)
    mixer_rows = lax.all_gather(normalize(my_stream, norm_gain), "tp", axis=0, tiled=True)

    def add_rows(shard_rows):
        return jnp.dot(mixer_rows, shard_rows, preferred_element_type=jnp.float32)

    gate = add_rows(lax.all_gather(gate_weight, "sp", axis=0, tiled=True))
    up_part = add_rows(lax.all_gather(up_weight, "sp", axis=0, tiled=True))
    hidden = (jax.nn.silu(gate) * up_part).astype(jnp.bfloat16)
    down_whole = lax.all_gather(down_weight, "sp", axis=1, tiled=True)
    down = lax.psum_scatter(
        jnp.dot(hidden, down_whole, preferred_element_type=jnp.float32).astype(jnp.bfloat16),
        "tp",
        scatter_dimension=0,
        tiled=True,
    ).astype(jnp.float32)
    return (my_stream.astype(jnp.float32) + 0.5 * down).astype(jnp.bfloat16)


SPLIT = 4


def fits(n_sp, kv_here, hidden_here):
    return n_sp % SPLIT == 0 and kv_here % SPLIT == 0 and hidden_here % (64 * SPLIT) == 0


def groups_of(n_sp):
    ranks = n_sp // SPLIT
    tokens = [[part * ranks + rank for part in range(SPLIT)] for rank in range(ranks)]
    hidden = [[part * ranks + rank for rank in range(ranks)] for part in range(SPLIT)]
    return tokens, hidden


MESH = pl.DeviceIdType.MESH


def layer_kernel(
    ranks,
    head_dim,
    kv_ref,
    q_ref,
    gu_ref,
    dn_ref,
    ow_ref,
    resid_ref,
    gain_ref,
    out_ref,
    kvb,
    qb,
    asend,
    ab,
    wgu,
    wdn,
    pj,
    prv,
    nb,
    st,
    dsb,
    drv,
    ds2,
    dzb,
    local_sem,
    kvz_s, kvz_r, kvx_s, kvx_r, q_s, q_r, gz_s, gz_r, dz_s, dz_r,
    gx_s, gx_r, dx_s, dx_r, gh_s, gh_r, dh_s, dh_r,
    at_s, at_r, pj_s, pj_r, nz_s, nz_r, np_s, np_r, dp_s, dp_r, fz_s, fz_r,
):
    sp = lax.axis_index("sp")
    core = lax.axis_index("tp")
    part = sp // ranks
    rank = sp % ranks
    rows = q_ref.shape[1]
    share = rows // 2
    depth = gu_ref.shape[1]
    width = dn_ref.shape[1]
    cols = dn_ref.shape[2]
    group = q_ref.shape[2] // head_dim
    other = 1 - core
    flips = (1, 2, 3)

    def flip(e):
        x = rank % 2
        y = rank // 2
        nx = 1 - x if e % 2 else x
        ny = 1 - y if e // 2 else y
        return ny * 2 + nx

    def peer_part(dz):
        return ((part + dz) % SPLIT) * ranks + rank

    def from_part(dz):
        return (part + SPLIT - dz) % SPLIT

    def near(e):
        return part * ranks + flip(e)

    sent = []

    def send(src, dst, s_sem, r_sem, target):
        copy = pltpu.make_async_remote_copy(
            src_ref=src, dst_ref=dst, send_sem=s_sem, recv_sem=r_sem, device_id=target, device_id_type=MESH
        )
        copy.start()
        sent.append(copy)

    def landed(dst, s_sem, r_sem):
        pltpu.make_async_remote_copy(
            src_ref=dst, dst_ref=dst, send_sem=s_sem, recv_sem=r_sem, device_id=(sp, other), device_id_type=MESH
        ).wait_recv()

    def gu_at(source, first=0, count=None):
        return wgu.at[pl.ds(pl.multiple_of(source * depth + first, 16), depth if count is None else count)]

    def dn_at(source, first=0, count=None):
        return wdn.at[pl.ds(first, width if count is None else count), pl.ds(pl.multiple_of(source * cols, cols), cols)]

    locals_ = [
        pltpu.make_async_copy(kv_ref.at[part], kvb.at[part, rank], local_sem.at[0]),
        pltpu.make_async_copy(q_ref.at[part], qb.at[part], local_sem.at[1]),
        pltpu.make_async_copy(gu_ref.at[part], gu_at(sp), local_sem.at[2]),
        pltpu.make_async_copy(dn_ref.at[part], dn_at(sp), local_sem.at[3]),
    ]
    for copy in locals_:
        copy.start()
    pad = wdn.shape[0] - width
    wdn[pl.ds(width, pad), :] = jnp.zeros((pad, wdn.shape[1]), wdn.dtype)

    barrier = pltpu.get_barrier_semaphore()
    for dz in range(1, SPLIT):
        pl.semaphore_signal(barrier, inc=1, device_id=(peer_part(dz), core), device_id_type=MESH)
    for e in flips:
        pl.semaphore_signal(barrier, inc=1, device_id=(near(e), core), device_id_type=MESH)
    pl.semaphore_signal(barrier, inc=1, device_id=(sp, other), device_id_type=MESH)
    pl.semaphore_wait(barrier, SPLIT - 1 + 3 + 1)

    def to_part(dz):
        return (part + dz) % SPLIT

    for dz in range(1, SPLIT):
        send(kv_ref.at[to_part(dz)], kvb.at[part, rank], kvz_s.at[dz], kvz_r.at[dz], (peer_part(dz), core))
    for e in flips:
        send(kv_ref.at[part], kvb.at[part, rank], kvx_s.at[0, e], kvx_r.at[0, e], (near(e), core))
    for dz in range(1, SPLIT):
        send(q_ref.at[to_part(dz)], qb.at[part], q_s.at[dz], q_r.at[dz], (peer_part(dz), core))
    for e in (1, 2):
        send(dn_ref.at[part], dn_at(sp), dx_s.at[0, e], dx_r.at[0, e], (near(e), core))
    for dz in range(1, SPLIT):
        send(gu_ref.at[to_part(dz)], gu_at(sp), gz_s.at[dz], gz_r.at[dz], (peer_part(dz), core))
        send(dn_ref.at[to_part(dz)], dn_at(sp), dz_s.at[dz], dz_r.at[dz], (peer_part(dz), core))
    for dz in range(1, SPLIT):
        slot = kvb.at[from_part(dz), rank]
        landed(slot, kvz_s.at[dz], kvz_r.at[dz])
        for e in flips:
            send(slot, slot, kvx_s.at[dz, e], kvx_r.at[dz, e], (near(e), core))
    for e in (1, 2):
        send(gu_ref.at[part], gu_at(sp), gx_s.at[0, e], gx_r.at[0, e], (near(e), core))

    def pass_on(dz):
        source = from_part(dz) * ranks + rank
        landed(gu_at(source), gz_s.at[dz], gz_r.at[dz])
        for e in (1, 2):
            send(gu_at(source), gu_at(source), gx_s.at[dz, e], gx_r.at[dz, e], (near(e), core))
        landed(dn_at(source), dz_s.at[dz], dz_r.at[dz])
        for e in (1, 2):
            send(dn_at(source), dn_at(source), dx_s.at[dz, e], dx_r.at[dz, e], (near(e), core))

    def halves(dz):
        for e in (1, 2):
            source = from_part(dz) * ranks + flip(e)
            across = (near(3 - e), core)
            landed(gu_at(source), gx_s.at[dz, e], gx_r.at[dz, e])
            half = gu_at(source, (e - 1) * depth // 2, depth // 2)
            send(half, half, gh_s.at[dz, e], gh_r.at[dz, e], across)
            landed(dn_at(source), dx_s.at[dz, e], dx_r.at[dz, e])
            half = dn_at(source, (e - 1) * width // 2, width // 2)
            send(half, half, dh_s.at[dz, e], dh_r.at[dz, e], across)

    for dz in range(SPLIT):
        for e in flips:
            landed(kvb.at[from_part(dz), flip(e)], kvx_s.at[dz, e], kvx_r.at[dz, e])
    locals_[0].wait()
    locals_[1].wait()
    for dz in range(1, SPLIT):
        landed(qb.at[from_part(dz)], q_s.at[dz], q_r.at[dz])

    factor = head_dim ** (-0.5) * math.log2(math.e)
    length = SPLIT * ranks * rows

    def attend(source, target):
        @pl.loop(0, group)
        def _(head):
            lanes = pl.ds(pl.multiple_of(head * head_dim, head_dim), head_dim)
            q = qb[source, :, lanes]
            keys = kvb[:, :, :, pl.ds(0, head_dim)].reshape(length, head_dim)
            scores = lax.dot_general(q, keys, (((1,), (1,)), ((), ())), preferred_element_type=jnp.float32)
            peak = jnp.max(scores, axis=-1, keepdims=True)
            weights = jnp.exp2((scores - peak) * factor)
            total = jnp.sum(weights, axis=-1, keepdims=True)
            vals = kvb[:, :, :, pl.ds(head_dim, head_dim)].reshape(length, head_dim)
            summed = jnp.dot(weights.astype(jnp.bfloat16), vals, preferred_element_type=jnp.float32)
            target[:, lanes] = (summed / total).astype(jnp.bfloat16)

    for dz in (1, 2, 3):
        attend(to_part(dz), asend.at[dz])
        send(asend.at[dz], ab.at[part], at_s.at[dz], at_r.at[dz], (peer_part(dz), core))
        if dz == 2:
            pass_on(1)
    attend(part, ab.at[part])
    halves(0)
    for dz in range(1, SPLIT):
        landed(ab.at[from_part(dz)], at_s.at[dz], at_r.at[dz])

    attn = jnp.concatenate([ab[index] for index in range(SPLIT)], axis=1)
    tile = 512
    for first in range(0, ow_ref.shape[1], tile):
        block = jnp.dot(attn, ow_ref[:, first : first + tile], preferred_element_type=jnp.float32)
        pj[:, :, first : first + tile] = block.astype(jnp.bfloat16).reshape(2, share, tile)
    send(pj.at[other], prv, pj_s, pj_r, (sp, other))
    pass_on(2)
    landed(prv, pj_s, pj_r)
    proj = pj[core].astype(jnp.float32) + prv[...].astype(jnp.float32)
    stream = (resid_ref[...].astype(jnp.float32) + proj).astype(jnp.bfloat16)
    st[...] = stream
    wide = stream.astype(jnp.float32)
    level = lax.rsqrt(jnp.mean(wide * wide, axis=-1, keepdims=True) + EPSILON)
    nb[part, core] = (wide * level * gain_ref[...]).astype(jnp.bfloat16)
    mine = nb.at[part, core]
    for dz in range(1, SPLIT):
        send(mine, mine, nz_s.at[dz], nz_r.at[dz], (peer_part(dz), core))
    send(mine, mine, np_s.at[0], np_r.at[0], (sp, other))
    halves(1)
    pass_on(3)
    halves(2)
    for dz in range(1, SPLIT):
        slot = nb.at[from_part(dz), core]
        landed(slot, nz_s.at[dz], nz_r.at[dz])
        send(slot, slot, np_s.at[dz], np_r.at[dz], (sp, other))
    halves(3)
    for dz in range(SPLIT):
        for e in (1, 2):
            source = from_part(dz) * ranks + flip(3)
            landed(gu_at(source, (e - 1) * depth // 2, depth // 2), gh_s.at[dz, e], gh_r.at[dz, e])
            landed(dn_at(source, (e - 1) * width // 2, width // 2), dh_s.at[dz, e], dh_r.at[dz, e])
    locals_[2].wait()
    locals_[3].wait()

    main = width // 128 * 128
    half_lane = width - main

    def feed(source, partner_sem):
        landed(nb.at[source, other], np_s.at[partner_sem], np_r.at[partner_sem])
        x = nb[source].reshape(rows, nb.shape[-1])
        pieces = []
        gate = jnp.dot(x, wgu[:, pl.ds(0, main)], preferred_element_type=jnp.float32)
        up = jnp.dot(x, wgu[:, pl.ds(main, main)], preferred_element_type=jnp.float32)
        pieces.append((gate / (1.0 + jnp.exp(-gate)) * up).astype(jnp.bfloat16))
        last = jnp.dot(x, wgu[:, pl.ds(2 * main, 128)], preferred_element_type=jnp.float32)
        turned = pltpu.roll(last, half_lane, 1)
        lane = lax.broadcasted_iota(jnp.int32, last.shape, 1)
        tail = jnp.where(lane < half_lane, last / (1.0 + jnp.exp(-last)) * turned, 0.0)
        pieces.append(tail.astype(jnp.bfloat16))
        hidden = jnp.concatenate(pieces, axis=1)
        for first in range(0, wdn.shape[1], tile):
            block = jnp.dot(hidden, wdn[:, first : first + tile], preferred_element_type=jnp.float32)
            dsb[source, :, :, first : first + tile] = block.astype(jnp.bfloat16).reshape(2, share, tile)

    def pair_up(dz):
        source = to_part(dz)
        landed(drv.at[dz], dp_s.at[dz], dp_r.at[dz])
        both = dsb[source, core].astype(jnp.float32) + drv[dz].astype(jnp.float32)
        if dz == 0:
            return both
        ds2[dz] = both.astype(jnp.bfloat16)
        send(ds2.at[dz], dzb.at[dz], fz_s.at[dz], fz_r.at[dz], (peer_part(dz), core))

    order = (1, 2, 3, 0)
    for place, dz in enumerate(order):
        feed(to_part(dz), (SPLIT - dz) % SPLIT)
        send(dsb.at[to_part(dz), other], drv.at[dz], dp_s.at[dz], dp_r.at[dz], (sp, other))
        if place:
            pair_up(order[place - 1])
    down = pair_up(0)
    for dz in range(1, SPLIT):
        landed(dzb.at[dz], fz_s.at[dz], fz_r.at[dz])
        down = down + dzb[dz].astype(jnp.float32)
    out_ref[...] = (st[...].astype(jnp.float32) + 0.5 * down).astype(jnp.bfloat16)
    for copy in sent:
        copy.wait_send()


def run_layer(kv, q, gate_up, down, out_weight, resid, gain, ranks, head_dim):
    rows = q.shape[1]
    share = rows // 2
    model = resid.shape[1]
    width = down.shape[1]
    n_sp = ranks * SPLIT
    half = jnp.bfloat16
    dma = pltpu.SemaphoreType.DMA
    per_part = [dma((SPLIT,))] * 2
    per_near = [dma((SPLIT, 4))] * 2
    anywhere = pl.BlockSpec(memory_space=pl.ANY)
    inside = pl.BlockSpec(memory_space=pltpu.VMEM)
    return pl.pallas_call(
        functools.partial(layer_kernel, ranks, head_dim),
        out_shape=jax.ShapeDtypeStruct((share, model), half),
        in_specs=[anywhere] * 4 + [inside] * 3,
        out_specs=inside,
        scratch_shapes=[
            pltpu.VMEM((SPLIT, ranks, rows, kv.shape[2]), half),
            pltpu.VMEM(q.shape, half),
            pltpu.VMEM(q.shape, half),
            pltpu.VMEM(q.shape, half),
            pltpu.VMEM((n_sp * gate_up.shape[1], gate_up.shape[2]), half),
            pltpu.VMEM((-(-width // 128) * 128, model), half),
            pltpu.VMEM((2, share, model), half),
            pltpu.VMEM((share, model), half),
            pltpu.VMEM((SPLIT, 2, share, model), half),
            pltpu.VMEM((share, model), half),
            pltpu.VMEM((SPLIT, 2, share, model), half),
            pltpu.VMEM((SPLIT, share, model), half),
            pltpu.VMEM((SPLIT, share, model), half),
            pltpu.VMEM((SPLIT, share, model), half),
            dma((4,)),
        ]
        + per_part + per_near + per_part * 3
        + per_near * 4
        + per_part + [dma, dma] + per_part * 4,
        compiler_params=pltpu.CompilerParams(
            collective_id=0, has_side_effects=True, vmem_limit_bytes=62 * 1024 * 1024
        ),
    )(kv, q, gate_up, down, out_weight, resid, gain)


def in_kernel(n_sp, n_tp, kv_here, head_dim, width):
    return n_sp == 4 * SPLIT and n_tp == 2 and kv_here == SPLIT and head_dim == 128 and width % 128 == 64


def body(
    resid,
    query,
    key,
    value,
    q_gain,
    k_gain,
    out_weight,
    norm_gain,
    gate_weight,
    up_weight,
    down_weight,
):
    rows = query.shape[0]
    head_dim = q_gain.shape[0]
    heads_here = query.shape[1] // head_dim
    kv_here = key.shape[1] // head_dim
    n_sp = lax.axis_size("sp")
    if not fits(n_sp, kv_here, gate_weight.shape[1]):
        return whole_body(
            resid, query, key, value, q_gain, k_gain, out_weight, norm_gain, gate_weight, up_weight, down_weight
        )
    tok_groups, hid_groups = groups_of(n_sp)
    ranks = n_sp // SPLIT
    group_size = heads_here // kv_here
    kv_part = kv_here // SPLIT

    def swap(array):
        return lax.all_to_all(array, "sp", 0, 0, axis_index_groups=tok_groups, tiled=True)

    def spread(array, axis):
        return lax.all_gather(array, "sp", axis=axis, axis_index_groups=hid_groups, tiled=True)

    positions = lax.axis_index("sp") * rows + jnp.arange(rows, dtype=jnp.int32)
    q_rot = prepare(query.reshape(rows, heads_here, head_dim), q_gain, positions)
    k_rot = prepare(key.reshape(rows, kv_here, head_dim), k_gain, positions)
    cut = lambda a: a.reshape(a.shape[0], SPLIT, -1).transpose(1, 0, 2).reshape(SPLIT * a.shape[0], -1)
    k_rot, val = cut(k_rot), cut(value)
    hidden_part = gate_weight.shape[1] // SPLIT
    if in_kernel(n_sp, lax.axis_size("tp"), kv_here, head_dim, hidden_part):
        stack = lambda a: a.reshape(SPLIT, a.shape[0] // SPLIT, -1)
        main = hidden_part // 128 * 128
        gate_cut, up_cut = stack(cut(gate_weight)), stack(cut(up_weight))
        gate_up = jnp.concatenate(
            [gate_cut[..., :main], up_cut[..., :main], gate_cut[..., main:], up_cut[..., main:]], axis=-1
        )
        share = rows // 2
        my_resid = lax.dynamic_slice_in_dim(resid, lax.axis_index("tp") * share, share, 0)
        return run_layer(
            stack(jnp.concatenate([k_rot, val], axis=1)),
            stack(cut(q_rot)),
            gate_up,
            stack(down_weight),
            out_weight,
            my_resid,
            norm_gain[None, :],
            ranks,
            head_dim,
        )
    pair = swap(jnp.concatenate([k_rot, val], axis=1))
    pair = spread(pair, 0)
    q_mine = swap(cut(q_rot))
    width = kv_part * head_dim
    keys = pair[:, :width].reshape(-1, kv_part, head_dim)
    vals = pair[:, width:].reshape(-1, kv_part, head_dim)
    grouped = q_mine.reshape(SPLIT * rows, kv_part, group_size, head_dim)
    gate_up = spread(swap(jnp.concatenate([cut(gate_weight), cut(up_weight)], axis=1)), 0)
    depth = gate_weight.shape[0]
    gate_up = gate_up.reshape(ranks, SPLIT, depth, -1).transpose(1, 0, 2, 3).reshape(n_sp * depth, -1)
    down_w = swap(down_weight)
    part = down_weight.shape[0] // SPLIT
    down_w = down_w.reshape(SPLIT, part, -1)
    down_w = lax.all_gather(down_w, "sp", axis=1, axis_index_groups=hid_groups)
    down_w = jnp.transpose(down_w, (2, 0, 1, 3)).reshape(part, -1)
    scores = jnp.einsum("qkgd,skd->kgqs", grouped, keys, preferred_element_type=jnp.float32) * head_dim ** (-0.5)
    weights = jnp.exp(scores - jnp.max(scores, axis=-1, keepdims=True))
    totals = jnp.sum(weights, axis=-1)
    accum = jnp.einsum("kgqs,skd->kgqd", weights.astype(jnp.bfloat16), vals, preferred_element_type=jnp.float32)
    attn = jnp.transpose(accum / totals[..., None], (2, 0, 1, 3)).astype(jnp.bfloat16).reshape(SPLIT * rows, -1)
    attn = swap(attn).reshape(SPLIT, rows, -1).transpose(1, 0, 2).reshape(rows, -1)
    return finish(attn, resid, out_weight, norm_gain, gate_up, down_w, tok_groups)


def finish(attn, resid, out_weight, norm_gain, gate_up, down_w, tok_groups):
    rows = resid.shape[0]
    n_tp = lax.axis_size("tp")
    share = rows // n_tp
    my_first = lax.axis_index("tp") * share
    proj = lax.psum_scatter(
        jnp.dot(attn, out_weight, preferred_element_type=jnp.float32).astype(jnp.bfloat16),
        "tp",
        scatter_dimension=0,
        tiled=True,
    ).astype(jnp.float32)
    my_resid = lax.dynamic_slice_in_dim(resid, my_first, share, 0)
    my_stream = (my_resid.astype(jnp.float32) + proj).astype(jnp.bfloat16)
    normed = normalize(my_stream, norm_gain)
    normed = lax.all_gather(normed, "sp", axis=0, axis_index_groups=tok_groups, tiled=False)
    normed = lax.all_gather(normed, "tp", axis=0, tiled=False)
    normed = normed.reshape(n_tp * SPLIT * share, -1)
    both = jnp.dot(normed, gate_up, preferred_element_type=jnp.float32)
    gate, up_part = jnp.split(both, 2, axis=1)
    hidden = (jax.nn.silu(gate) * up_part).astype(jnp.bfloat16)
    down = jnp.dot(hidden, down_w, preferred_element_type=jnp.float32).astype(jnp.bfloat16)
    down = lax.psum_scatter(down, "tp", scatter_dimension=0, tiled=True)
    down = lax.all_to_all(
        down.reshape(SPLIT, share, -1), "sp", 0, 0, axis_index_groups=tok_groups, tiled=True
    )
    down = jnp.sum(down.astype(jnp.float32), axis=0)
    return (my_stream.astype(jnp.float32) + 0.5 * down).astype(jnp.bfloat16)


def solution(mesh):
    placed = (
        P("sp", None),
        P("sp", "tp"),
        P("sp", "tp"),
        P("sp", "tp"),
        P(),
        P(),
        P("tp", None),
        P(),
        P("sp", "tp"),
        P("sp", "tp"),
        P("tp", "sp"),
    )
    return jax.shard_map(
        body, mesh=mesh, in_specs=placed, out_specs=P(("sp", "tp"), None), check_vma=False
    )
```

```python
import functools
import math

import jax
import jax.numpy as jnp
from jax import lax
from jax.experimental import pallas as pl
from jax.experimental.pallas import tpu as pltpu
from jax.sharding import PartitionSpec as P

GRID_W = 64


EPSILON = 1e-06


def rotate(values, positions):
    dim_size = values.shape[-1]
    half_dim = dim_size // 2
    quarter = half_dim // 2
    inverse = 10000.0 ** (-jnp.arange(quarter, dtype=jnp.float32) / quarter)
    outputs = []
    for axis_pos, coords in enumerate((positions // GRID_W, positions % GRID_W)):
        angles = coords.astype(jnp.float32)[:, None] * inverse[None, :]
        cosine = jnp.cos(angles)[:, None, :]
        sine = jnp.sin(angles)[:, None, :]
        section = values[..., axis_pos * half_dim : (axis_pos + 1) * half_dim]
        first_half = section[..., :quarter]
        second_half = section[..., quarter:]
        outputs += [
            first_half * cosine - second_half * sine,
            second_half * cosine + first_half * sine,
        ]
    return jnp.concatenate(outputs, axis=-1)


def prepare(projected, gain, positions):
    values = projected.astype(jnp.float32)
    normed = values * lax.rsqrt(jnp.mean(values * values, axis=-1, keepdims=True) + EPSILON) * gain
    return rotate(normed, positions).astype(jnp.bfloat16)


def normalize(stream, gain):
    values = stream.astype(jnp.float32)
    return (
        values * lax.rsqrt(jnp.mean(values * values, axis=-1, keepdims=True) + EPSILON) * gain
    ).astype(jnp.bfloat16)


def whole_body(
    resid,
    query,
    key,
    value,
    q_gain,
    k_gain,
    out_weight,
    norm_gain,
    gate_weight,
    up_weight,
    down_weight,
):
    rows_here = query.shape[0]
    head_dim = q_gain.shape[0]
    heads_here = query.shape[1] // head_dim
    kv_here = key.shape[1] // head_dim
    group_size = heads_here // kv_here
    score_scale = head_dim ** (-0.5)
    positions = lax.axis_index("sp") * rows_here + jnp.arange(rows_here, dtype=jnp.int32)
    q_rot = prepare(query.reshape(rows_here, heads_here, head_dim), q_gain, positions)
    k_rot = prepare(key.reshape(rows_here, kv_here, head_dim), k_gain, positions)
    val_rows = value.reshape(rows_here, kv_here, head_dim)
    grouped = q_rot.reshape(rows_here, kv_here, group_size, head_dim)

    def key_block(carry, block):
        maxima, totals, accum = carry
        block_keys, block_vals = block
        scores = (
            jnp.einsum("qkgd,skd->kgqs", grouped, block_keys, preferred_element_type=jnp.float32)
            * score_scale
        )
        new_max = jnp.maximum(maxima, jnp.max(scores, axis=-1))
        shrink = jnp.exp(maxima - new_max)
        weights = jnp.exp(scores - new_max[..., None])
        totals = totals * shrink + jnp.sum(weights, axis=-1)
        accum = accum * shrink[..., None] + jnp.einsum(
            "kgqs,skd->kgqd",
            weights.astype(jnp.bfloat16),
            block_vals,
            preferred_element_type=jnp.float32,
        )
        return ((new_max, totals, accum), None)

    start_max = jnp.full((kv_here, group_size, rows_here), -1e30, jnp.float32)
    start_total = jnp.zeros((kv_here, group_size, rows_here), jnp.float32)
    start_accum = jnp.zeros((kv_here, group_size, rows_here, head_dim), jnp.float32)
    carry = (start_max, start_total, start_accum)
    key_part = lax.all_gather(k_rot, "sp", axis=0, tiled=True)
    val_part = lax.all_gather(val_rows, "sp", axis=0, tiled=True)
    length = key_part.shape[0]
    factor = 4
    span = rows_here * factor
    turns = length // span
    key_blocks = key_part.reshape(turns, span, kv_here, head_dim)
    val_blocks = val_part.reshape(turns, span, kv_here, head_dim)
    carry, _ = lax.scan(key_block, carry, (key_blocks, val_blocks))
    maxima, totals, accum = carry
    attn = (
        jnp.transpose(accum / totals[..., None], (2, 0, 1, 3))
        .reshape(rows_here, heads_here * head_dim)
        .astype(jnp.bfloat16)
    )
    share = rows_here // lax.axis_size("tp")
    my_first = lax.axis_index("tp") * share
    proj = lax.psum_scatter(
        jnp.dot(attn, out_weight, preferred_element_type=jnp.float32).astype(jnp.bfloat16),
        "tp",
        scatter_dimension=0,
        tiled=True,
    ).astype(jnp.float32)
    my_resid = lax.dynamic_slice_in_dim(resid, my_first, share, 0)
    my_stream = (my_resid.astype(jnp.float32) + proj).astype(jnp.bfloat16)
    mixer_rows = lax.all_gather(normalize(my_stream, norm_gain), "tp", axis=0, tiled=True)

    def add_rows(shard_rows):
        return jnp.dot(mixer_rows, shard_rows, preferred_element_type=jnp.float32)

    gate = add_rows(lax.all_gather(gate_weight, "sp", axis=0, tiled=True))
    up_part = add_rows(lax.all_gather(up_weight, "sp", axis=0, tiled=True))
    hidden = (jax.nn.silu(gate) * up_part).astype(jnp.bfloat16)
    down_whole = lax.all_gather(down_weight, "sp", axis=1, tiled=True)
    down = lax.psum_scatter(
        jnp.dot(hidden, down_whole, preferred_element_type=jnp.float32).astype(jnp.bfloat16),
        "tp",
        scatter_dimension=0,
        tiled=True,
    ).astype(jnp.float32)
    return (my_stream.astype(jnp.float32) + 0.5 * down).astype(jnp.bfloat16)


SPLIT = 4


def fits(n_sp, kv_here, hidden_here):
    return n_sp % SPLIT == 0 and kv_here % SPLIT == 0 and hidden_here % (64 * SPLIT) == 0


def groups_of(n_sp):
    ranks = n_sp // SPLIT
    tokens = [[part * ranks + rank for part in range(SPLIT)] for rank in range(ranks)]
    hidden = [[part * ranks + rank for rank in range(ranks)] for part in range(SPLIT)]
    return tokens, hidden


MESH = pl.DeviceIdType.MESH


def layer_kernel(
    ranks,
    head_dim,
    kv_ref,
    q_ref,
    gu_ref,
    dn_ref,
    ow_ref,
    resid_ref,
    gain_ref,
    out_ref,
    kvb,
    qb,
    asend,
    ab,
    wgu,
    wdn,
    pj,
    prv,
    nb,
    st,
    dsb,
    drv,
    ds2,
    dzb,
    acc,
    local_sem,
    kvz_s, kvz_r, kvx_s, kvx_r, q_s, q_r, gz_s, gz_r, dz_s, dz_r,
    gx_s, gx_r, dx_s, dx_r, gh_s, gh_r, dh_s, dh_r,
    at_s, at_r, pj_s, pj_r, nz_s, nz_r, np_s, np_r, dp_s, dp_r, fz_s, fz_r,
):
    sp = lax.axis_index("sp")
    core = lax.axis_index("tp")
    part = sp // ranks
    rank = sp % ranks
    rows = q_ref.shape[1]
    share = rows // 2
    depth = gu_ref.shape[1]
    width = dn_ref.shape[1]
    cols = dn_ref.shape[2]
    group = q_ref.shape[2] // head_dim
    other = 1 - core
    flips = (1, 2, 3)

    def flip(e):
        x = rank % 2
        y = rank // 2
        nx = 1 - x if e % 2 else x
        ny = 1 - y if e // 2 else y
        return ny * 2 + nx

    def peer_part(dz):
        return ((part + dz) % SPLIT) * ranks + rank

    def from_part(dz):
        return (part + SPLIT - dz) % SPLIT

    def near(e):
        return part * ranks + flip(e)

    sent = []

    def send(src, dst, s_sem, r_sem, target, keep=True):
        copy = pltpu.make_async_remote_copy(
            src_ref=src, dst_ref=dst, send_sem=s_sem, recv_sem=r_sem, device_id=target, device_id_type=MESH
        )
        copy.start()
        if keep:
            sent.append(copy)
        return copy

    def landed(dst, s_sem, r_sem):
        pltpu.make_async_remote_copy(
            src_ref=dst, dst_ref=dst, send_sem=s_sem, recv_sem=r_sem, device_id=(sp, other), device_id_type=MESH
        ).wait_recv()

    def gu_at(source, first=0, count=None):
        return wgu.at[pl.ds(pl.multiple_of(source * depth + first, 16), depth if count is None else count)]

    def dn_at(source, first=0, count=None):
        return wdn.at[pl.ds(first, width if count is None else count), pl.ds(pl.multiple_of(source * cols, cols), cols)]

    locals_ = [
        pltpu.make_async_copy(kv_ref.at[part], kvb.at[part, rank], local_sem.at[0]),
        pltpu.make_async_copy(q_ref.at[part], qb.at[part], local_sem.at[1]),
        pltpu.make_async_copy(gu_ref.at[part], gu_at(sp), local_sem.at[2]),
        pltpu.make_async_copy(dn_ref.at[part], dn_at(sp), local_sem.at[3]),
    ]
    for copy in locals_:
        copy.start()
    pad = wdn.shape[0] - width
    wdn[pl.ds(width, pad), :] = jnp.zeros((pad, wdn.shape[1]), wdn.dtype)

    barrier = pltpu.get_barrier_semaphore()
    for dz in range(1, SPLIT):
        pl.semaphore_signal(barrier, inc=1, device_id=(peer_part(dz), core), device_id_type=MESH)
    for e in flips:
        pl.semaphore_signal(barrier, inc=1, device_id=(near(e), core), device_id_type=MESH)
    pl.semaphore_signal(barrier, inc=1, device_id=(sp, other), device_id_type=MESH)
    pl.semaphore_wait(barrier, SPLIT - 1 + 3 + 1)

    def to_part(dz):
        return (part + dz) % SPLIT

    for dz in range(1, SPLIT):
        send(kv_ref.at[to_part(dz)], kvb.at[part, rank], kvz_s.at[dz], kvz_r.at[dz], (peer_part(dz), core))
    for e in flips:
        send(kv_ref.at[part], kvb.at[part, rank], kvx_s.at[0, e], kvx_r.at[0, e], (near(e), core))
    for dz in range(1, SPLIT):
        send(q_ref.at[to_part(dz)], qb.at[part], q_s.at[dz], q_r.at[dz], (peer_part(dz), core))
    for e in (1, 2):
        send(dn_ref.at[part], dn_at(sp), dx_s.at[0, e], dx_r.at[0, e], (near(e), core))
    for dz in range(1, SPLIT):
        send(gu_ref.at[to_part(dz)], gu_at(sp), gz_s.at[dz], gz_r.at[dz], (peer_part(dz), core))
        send(dn_ref.at[to_part(dz)], dn_at(sp), dz_s.at[dz], dz_r.at[dz], (peer_part(dz), core))
    for dz in range(1, SPLIT):
        slot = kvb.at[from_part(dz), rank]
        landed(slot, kvz_s.at[dz], kvz_r.at[dz])
        for e in flips:
            send(slot, slot, kvx_s.at[dz, e], kvx_r.at[dz, e], (near(e), core))
    for e in (1, 2):
        send(gu_ref.at[part], gu_at(sp), gx_s.at[0, e], gx_r.at[0, e], (near(e), core))

    def pass_on(dz):
        source = from_part(dz) * ranks + rank
        landed(gu_at(source), gz_s.at[dz], gz_r.at[dz])
        for e in (1, 2):
            send(gu_at(source), gu_at(source), gx_s.at[dz, e], gx_r.at[dz, e], (near(e), core))
        landed(dn_at(source), dz_s.at[dz], dz_r.at[dz])
        for e in (1, 2):
            send(dn_at(source), dn_at(source), dx_s.at[dz, e], dx_r.at[dz, e], (near(e), core))

    def halves(dz):
        for e in (1, 2):
            source = from_part(dz) * ranks + flip(e)
            across = (near(3 - e), core)
            landed(gu_at(source), gx_s.at[dz, e], gx_r.at[dz, e])
            half = gu_at(source, (e - 1) * depth // 2, depth // 2)
            send(half, half, gh_s.at[dz, e], gh_r.at[dz, e], across)
            landed(dn_at(source), dx_s.at[dz, e], dx_r.at[dz, e])
            half = dn_at(source, (e - 1) * width // 2, width // 2)
            send(half, half, dh_s.at[dz, e], dh_r.at[dz, e], across)

    for dz in range(SPLIT):
        for e in flips:
            landed(kvb.at[from_part(dz), flip(e)], kvx_s.at[dz, e], kvx_r.at[dz, e])
    locals_[0].wait()
    locals_[1].wait()
    for dz in range(1, SPLIT):
        landed(qb.at[from_part(dz)], q_s.at[dz], q_r.at[dz])

    factor = head_dim ** (-0.5) * math.log2(math.e)
    length = SPLIT * ranks * rows

    def attend(source, target):
        @pl.loop(0, group)
        def _(head):
            lanes = pl.ds(pl.multiple_of(head * head_dim, head_dim), head_dim)
            q = qb[source, :, lanes]
            keys = kvb[:, :, :, pl.ds(0, head_dim)].reshape(length, head_dim)
            scores = lax.dot_general(q, keys, (((1,), (1,)), ((), ())), preferred_element_type=jnp.float32)
            peak = jnp.max(scores, axis=-1, keepdims=True)
            weights = jnp.exp2((scores - peak) * factor)
            total = jnp.sum(weights, axis=-1, keepdims=True)
            vals = kvb[:, :, :, pl.ds(head_dim, head_dim)].reshape(length, head_dim)
            summed = jnp.dot(weights.astype(jnp.bfloat16), vals, preferred_element_type=jnp.float32)
            target[:, lanes] = (summed / total).astype(jnp.bfloat16)

    for dz in (1, 2, 3):
        attend(to_part(dz), asend.at[dz])
        send(asend.at[dz], ab.at[part], at_s.at[dz], at_r.at[dz], (peer_part(dz), core))
        if dz == 2:
            pass_on(1)
    attend(part, ab.at[part])
    halves(0)
    for dz in range(1, SPLIT):
        landed(ab.at[from_part(dz)], at_s.at[dz], at_r.at[dz])

    attn = jnp.concatenate([ab[index] for index in range(SPLIT)], axis=1)
    tile = 512
    for first in range(0, ow_ref.shape[1], tile):
        block = jnp.dot(attn, ow_ref[:, first : first + tile], preferred_element_type=jnp.float32)
        pj[:, :, first : first + tile] = block.astype(jnp.bfloat16).reshape(2, share, tile)
    send(pj.at[other], prv, pj_s, pj_r, (sp, other))
    pass_on(2)
    landed(prv, pj_s, pj_r)
    proj = pj[core].astype(jnp.float32) + prv[...].astype(jnp.float32)
    stream = (resid_ref[...].astype(jnp.float32) + proj).astype(jnp.bfloat16)
    st[...] = stream
    wide = stream.astype(jnp.float32)
    level = lax.rsqrt(jnp.mean(wide * wide, axis=-1, keepdims=True) + EPSILON)
    nb[part, core] = (wide * level * gain_ref[...]).astype(jnp.bfloat16)
    ahead = [(part < SPLIT - 1, sp + ranks, -1), (part > 0, sp - ranks, 1)]

    def step_on(source, step, way):
        slot = nb.at[source, core]
        go, target, _ = ahead[way]

        @pl.when(go)
        def _():
            send(slot, slot, nz_s.at[way, step], nz_r.at[way, step], (target, core), keep=False)

    def present(way, step):
        source = part + ahead[way][2] * (step + 1)
        return source, (source >= 0) & (source < SPLIT)

    step_on(part, 0, 0)
    step_on(part, 0, 1)
    mine = nb.at[part, core]
    send(mine, mine, np_s.at[part], np_r.at[part], (sp, other))
    def hop(step):
        for way in (0, 1):
            source, there = present(way, step)

            @pl.when(there)
            def _():
                slot = nb.at[source, core]
                landed(slot, nz_s.at[way, step], nz_r.at[way, step])
                if step < SPLIT - 2:
                    step_on(source, step + 1, way)
                send(slot, slot, np_s.at[source], np_r.at[source], (sp, other), keep=False)

    halves(1)
    pass_on(3)
    hop(0)
    halves(2)
    hop(1)
    halves(3)
    hop(2)
    for dz in range(SPLIT):
        for e in (1, 2):
            source = from_part(dz) * ranks + flip(3)
            landed(gu_at(source, (e - 1) * depth // 2, depth // 2), gh_s.at[dz, e], gh_r.at[dz, e])
            landed(dn_at(source, (e - 1) * width // 2, width // 2), dh_s.at[dz, e], dh_r.at[dz, e])
    locals_[2].wait()
    locals_[3].wait()

    main = width // 128 * 128
    half_lane = width - main

    def feed(source):
        landed(nb.at[source, other], np_s.at[source], np_r.at[source])
        x = nb[source].reshape(rows, nb.shape[-1])
        pieces = []
        gate = jnp.dot(x, wgu[:, pl.ds(0, main)], preferred_element_type=jnp.float32)
        up = jnp.dot(x, wgu[:, pl.ds(main, main)], preferred_element_type=jnp.float32)
        pieces.append((gate / (1.0 + jnp.exp(-gate)) * up).astype(jnp.bfloat16))
        last = jnp.dot(x, wgu[:, pl.ds(2 * main, 128)], preferred_element_type=jnp.float32)
        turned = pltpu.roll(last, half_lane, 1)
        lane = lax.broadcasted_iota(jnp.int32, last.shape, 1)
        tail = jnp.where(lane < half_lane, last / (1.0 + jnp.exp(-last)) * turned, 0.0)
        pieces.append(tail.astype(jnp.bfloat16))
        hidden = jnp.concatenate(pieces, axis=1)
        for first in range(0, wdn.shape[1], tile):
            block = jnp.dot(hidden, wdn[:, first : first + tile], preferred_element_type=jnp.float32)
            dsb[source, :, :, first : first + tile] = block.astype(jnp.bfloat16).reshape(2, share, tile)

    high, odd = part // 2, part % 2
    order = (3 - 3 * high, 2 - 2 * odd + high, 1 + odd, part)
    at_end = (part == 0) | (part == SPLIT - 1)
    inner = (part > 0) & (part < SPLIT - 1)

    def pair_sum(place):
        landed(drv.at[place], dp_s.at[place], dp_r.at[place])
        return dsb[order[place], core].astype(jnp.float32) + drv[place].astype(jnp.float32)

    def onward(place, first):
        target = order[place]
        way = 1 - (target > part).astype(jnp.int32)
        total = pair_sum(place)
        if not first:
            landed(dzb.at[way, target], fz_s.at[way, target], fz_r.at[way, target])
            total = total + dzb[way, target].astype(jnp.float32)
        ds2[target] = total.astype(jnp.bfloat16)
        slot = dzb.at[way, target]
        sender = fz_s.at[way, target]
        send(ds2.at[target], slot, sender, fz_r.at[way, target], (sp + ranks * (1 - 2 * way), core), keep=False)

    for place in range(SPLIT):
        feed(order[place])
        send(dsb.at[order[place], other], drv.at[place], dp_s.at[place], dp_r.at[place], (sp, other))
        if place:

            @pl.when(at_end)
            def _():
                onward(place - 1, True)

    @pl.when(inner)
    def _():
        for place in range(SPLIT - 1):
            onward(place, False)

    acc[...] = pair_sum(SPLIT - 1)
    for way, some in ((0, part > 0), (1, part < SPLIT - 1)):

        @pl.when(some)
        def _():
            landed(dzb.at[way, part], fz_s.at[way, part], fz_r.at[way, part])
            acc[...] += dzb[way, part].astype(jnp.float32)

    down = acc[...]
    out_ref[...] = (st[...].astype(jnp.float32) + 0.5 * down).astype(jnp.bfloat16)
    for copy in sent:
        copy.wait_send()

    def left(src, s_sem, r_sem):
        pltpu.make_async_remote_copy(
            src_ref=src, dst_ref=src, send_sem=s_sem, recv_sem=r_sem, device_id=(sp, other), device_id_type=MESH
        ).wait_send()

    for way in (0, 1):
        for step in range(SPLIT - 1):
            source, there = present(way, step)

            @pl.when(there)
            def _():
                left(nb.at[source, core], np_s.at[source], np_r.at[source])

        for step in range(SPLIT - 1):
            source = part + ahead[way][2] * step

            @pl.when(ahead[way][0] & (source >= 0) & (source < SPLIT))
            def _():
                left(nb.at[source, core], nz_s.at[way, step], nz_r.at[way, step])

    for place in range(SPLIT - 1):
        target = order[place]
        way = 1 - (target > part).astype(jnp.int32)
        left(ds2.at[target], fz_s.at[way, target], fz_r.at[way, target])


def run_layer(kv, q, gate_up, down, out_weight, resid, gain, ranks, head_dim):
    rows = q.shape[1]
    share = rows // 2
    model = resid.shape[1]
    width = down.shape[1]
    n_sp = ranks * SPLIT
    half = jnp.bfloat16
    dma = pltpu.SemaphoreType.DMA
    per_part = [dma((SPLIT,))] * 2
    per_near = [dma((SPLIT, 4))] * 2
    per_way = [dma((2, SPLIT))] * 2
    anywhere = pl.BlockSpec(memory_space=pl.ANY)
    inside = pl.BlockSpec(memory_space=pltpu.VMEM)
    return pl.pallas_call(
        functools.partial(layer_kernel, ranks, head_dim),
        out_shape=jax.ShapeDtypeStruct((share, model), half),
        in_specs=[anywhere] * 4 + [inside] * 3,
        out_specs=inside,
        scratch_shapes=[
            pltpu.VMEM((SPLIT, ranks, rows, kv.shape[2]), half),
            pltpu.VMEM(q.shape, half),
            pltpu.VMEM(q.shape, half),
            pltpu.VMEM(q.shape, half),
            pltpu.VMEM((n_sp * gate_up.shape[1], gate_up.shape[2]), half),
            pltpu.VMEM((-(-width // 128) * 128, model), half),
            pltpu.VMEM((2, share, model), half),
            pltpu.VMEM((share, model), half),
            pltpu.VMEM((SPLIT, 2, share, model), half),
            pltpu.VMEM((share, model), half),
            pltpu.VMEM((SPLIT, 2, share, model), half),
            pltpu.VMEM((SPLIT, share, model), half),
            pltpu.VMEM((SPLIT, share, model), half),
            pltpu.VMEM((2, SPLIT, share, model), half),
            pltpu.VMEM((share, model), jnp.float32),
            dma((4,)),
        ]
        + per_part + per_near + per_part * 3
        + per_near * 4
        + per_part + [dma, dma] + per_way + per_part * 2 + per_way,
        compiler_params=pltpu.CompilerParams(
            collective_id=0, has_side_effects=True, vmem_limit_bytes=62 * 1024 * 1024
        ),
    )(kv, q, gate_up, down, out_weight, resid, gain)


def in_kernel(n_sp, n_tp, kv_here, head_dim, width):
    return n_sp == 4 * SPLIT and n_tp == 2 and kv_here == SPLIT and head_dim == 128 and width % 128 == 64


def body(
    resid,
    query,
    key,
    value,
    q_gain,
    k_gain,
    out_weight,
    norm_gain,
    gate_weight,
    up_weight,
    down_weight,
):
    rows = query.shape[0]
    head_dim = q_gain.shape[0]
    heads_here = query.shape[1] // head_dim
    kv_here = key.shape[1] // head_dim
    n_sp = lax.axis_size("sp")
    if not fits(n_sp, kv_here, gate_weight.shape[1]):
        return whole_body(
            resid, query, key, value, q_gain, k_gain, out_weight, norm_gain, gate_weight, up_weight, down_weight
        )
    tok_groups, hid_groups = groups_of(n_sp)
    ranks = n_sp // SPLIT
    group_size = heads_here // kv_here
    kv_part = kv_here // SPLIT

    def swap(array):
        return lax.all_to_all(array, "sp", 0, 0, axis_index_groups=tok_groups, tiled=True)

    def spread(array, axis):
        return lax.all_gather(array, "sp", axis=axis, axis_index_groups=hid_groups, tiled=True)

    positions = lax.axis_index("sp") * rows + jnp.arange(rows, dtype=jnp.int32)
    q_rot = prepare(query.reshape(rows, heads_here, head_dim), q_gain, positions)
    k_rot = prepare(key.reshape(rows, kv_here, head_dim), k_gain, positions)
    cut = lambda a: a.reshape(a.shape[0], SPLIT, -1).transpose(1, 0, 2).reshape(SPLIT * a.shape[0], -1)
    k_rot, val = cut(k_rot), cut(value)
    hidden_part = gate_weight.shape[1] // SPLIT
    if in_kernel(n_sp, lax.axis_size("tp"), kv_here, head_dim, hidden_part):
        stack = lambda a: a.reshape(SPLIT, a.shape[0] // SPLIT, -1)
        main = hidden_part // 128 * 128
        gate_cut, up_cut = stack(cut(gate_weight)), stack(cut(up_weight))
        gate_up = jnp.concatenate(
            [gate_cut[..., :main], up_cut[..., :main], gate_cut[..., main:], up_cut[..., main:]], axis=-1
        )
        share = rows // 2
        my_resid = lax.dynamic_slice_in_dim(resid, lax.axis_index("tp") * share, share, 0)
        return run_layer(
            stack(jnp.concatenate([k_rot, val], axis=1)),
            stack(cut(q_rot)),
            gate_up,
            stack(down_weight),
            out_weight,
            my_resid,
            norm_gain[None, :],
            ranks,
            head_dim,
        )
    pair = swap(jnp.concatenate([k_rot, val], axis=1))
    pair = spread(pair, 0)
    q_mine = swap(cut(q_rot))
    width = kv_part * head_dim
    keys = pair[:, :width].reshape(-1, kv_part, head_dim)
    vals = pair[:, width:].reshape(-1, kv_part, head_dim)
    grouped = q_mine.reshape(SPLIT * rows, kv_part, group_size, head_dim)
    gate_up = spread(swap(jnp.concatenate([cut(gate_weight), cut(up_weight)], axis=1)), 0)
    depth = gate_weight.shape[0]
    gate_up = gate_up.reshape(ranks, SPLIT, depth, -1).transpose(1, 0, 2, 3).reshape(n_sp * depth, -1)
    down_w = swap(down_weight)
    part = down_weight.shape[0] // SPLIT
    down_w = down_w.reshape(SPLIT, part, -1)
    down_w = lax.all_gather(down_w, "sp", axis=1, axis_index_groups=hid_groups)
    down_w = jnp.transpose(down_w, (2, 0, 1, 3)).reshape(part, -1)
    scores = jnp.einsum("qkgd,skd->kgqs", grouped, keys, preferred_element_type=jnp.float32) * head_dim ** (-0.5)
    weights = jnp.exp(scores - jnp.max(scores, axis=-1, keepdims=True))
    totals = jnp.sum(weights, axis=-1)
    accum = jnp.einsum("kgqs,skd->kgqd", weights.astype(jnp.bfloat16), vals, preferred_element_type=jnp.float32)
    attn = jnp.transpose(accum / totals[..., None], (2, 0, 1, 3)).astype(jnp.bfloat16).reshape(SPLIT * rows, -1)
    attn = swap(attn).reshape(SPLIT, rows, -1).transpose(1, 0, 2).reshape(rows, -1)
    return finish(attn, resid, out_weight, norm_gain, gate_up, down_w, tok_groups)


def finish(attn, resid, out_weight, norm_gain, gate_up, down_w, tok_groups):
    rows = resid.shape[0]
    n_tp = lax.axis_size("tp")
    share = rows // n_tp
    my_first = lax.axis_index("tp") * share
    proj = lax.psum_scatter(
        jnp.dot(attn, out_weight, preferred_element_type=jnp.float32).astype(jnp.bfloat16),
        "tp",
        scatter_dimension=0,
        tiled=True,
    ).astype(jnp.float32)
    my_resid = lax.dynamic_slice_in_dim(resid, my_first, share, 0)
    my_stream = (my_resid.astype(jnp.float32) + proj).astype(jnp.bfloat16)
    normed = normalize(my_stream, norm_gain)
    normed = lax.all_gather(normed, "sp", axis=0, axis_index_groups=tok_groups, tiled=False)
    normed = lax.all_gather(normed, "tp", axis=0, tiled=False)
    normed = normed.reshape(n_tp * SPLIT * share, -1)
    both = jnp.dot(normed, gate_up, preferred_element_type=jnp.float32)
    gate, up_part = jnp.split(both, 2, axis=1)
    hidden = (jax.nn.silu(gate) * up_part).astype(jnp.bfloat16)
    down = jnp.dot(hidden, down_w, preferred_element_type=jnp.float32).astype(jnp.bfloat16)
    down = lax.psum_scatter(down, "tp", scatter_dimension=0, tiled=True)
    down = lax.all_to_all(
        down.reshape(SPLIT, share, -1), "sp", 0, 0, axis_index_groups=tok_groups, tiled=True
    )
    down = jnp.sum(down.astype(jnp.float32), axis=0)
    return (my_stream.astype(jnp.float32) + 0.5 * down).astype(jnp.bfloat16)


def solution(mesh):
    placed = (
        P("sp", None),
        P("sp", "tp"),
        P("sp", "tp"),
        P("sp", "tp"),
        P(),
        P(),
        P("tp", None),
        P(),
        P("sp", "tp"),
        P("sp", "tp"),
        P("tp", "sp"),
    )
    return jax.shard_map(
        body, mesh=mesh, in_specs=placed, out_specs=P(("sp", "tp"), None), check_vma=False
    )
```

```python
import functools
import math

import jax
import jax.numpy as jnp
import numpy as np
from jax import lax
from jax.experimental import pallas as pl
from jax.experimental.pallas import tpu as pltpu
from jax.sharding import PartitionSpec as P

GRID_W = 64


EPSILON = 1e-06


def rotate(values, positions):
    dim_size = values.shape[-1]
    half_dim = dim_size // 2
    quarter = half_dim // 2
    inverse = 10000.0 ** (-jnp.arange(quarter, dtype=jnp.float32) / quarter)
    outputs = []
    for axis_pos, coords in enumerate((positions // GRID_W, positions % GRID_W)):
        angles = coords.astype(jnp.float32)[:, None] * inverse[None, :]
        cosine = jnp.cos(angles)[:, None, :]
        sine = jnp.sin(angles)[:, None, :]
        section = values[..., axis_pos * half_dim : (axis_pos + 1) * half_dim]
        first_half = section[..., :quarter]
        second_half = section[..., quarter:]
        outputs += [
            first_half * cosine - second_half * sine,
            second_half * cosine + first_half * sine,
        ]
    return jnp.concatenate(outputs, axis=-1)


def prepare(projected, gain, positions):
    values = projected.astype(jnp.float32)
    normed = values * lax.rsqrt(jnp.mean(values * values, axis=-1, keepdims=True) + EPSILON) * gain
    return rotate(normed, positions).astype(jnp.bfloat16)


def normalize(stream, gain):
    values = stream.astype(jnp.float32)
    return (
        values * lax.rsqrt(jnp.mean(values * values, axis=-1, keepdims=True) + EPSILON) * gain
    ).astype(jnp.bfloat16)


def whole_body(
    resid,
    query,
    key,
    value,
    q_gain,
    k_gain,
    out_weight,
    norm_gain,
    gate_weight,
    up_weight,
    down_weight,
):
    rows_here = query.shape[0]
    head_dim = q_gain.shape[0]
    heads_here = query.shape[1] // head_dim
    kv_here = key.shape[1] // head_dim
    group_size = heads_here // kv_here
    score_scale = head_dim ** (-0.5)
    positions = lax.axis_index("sp") * rows_here + jnp.arange(rows_here, dtype=jnp.int32)
    q_rot = prepare(query.reshape(rows_here, heads_here, head_dim), q_gain, positions)
    k_rot = prepare(key.reshape(rows_here, kv_here, head_dim), k_gain, positions)
    val_rows = value.reshape(rows_here, kv_here, head_dim)
    grouped = q_rot.reshape(rows_here, kv_here, group_size, head_dim)

    def key_block(carry, block):
        maxima, totals, accum = carry
        block_keys, block_vals = block
        scores = (
            jnp.einsum("qkgd,skd->kgqs", grouped, block_keys, preferred_element_type=jnp.float32)
            * score_scale
        )
        new_max = jnp.maximum(maxima, jnp.max(scores, axis=-1))
        shrink = jnp.exp(maxima - new_max)
        weights = jnp.exp(scores - new_max[..., None])
        totals = totals * shrink + jnp.sum(weights, axis=-1)
        accum = accum * shrink[..., None] + jnp.einsum(
            "kgqs,skd->kgqd",
            weights.astype(jnp.bfloat16),
            block_vals,
            preferred_element_type=jnp.float32,
        )
        return ((new_max, totals, accum), None)

    start_max = jnp.full((kv_here, group_size, rows_here), -1e30, jnp.float32)
    start_total = jnp.zeros((kv_here, group_size, rows_here), jnp.float32)
    start_accum = jnp.zeros((kv_here, group_size, rows_here, head_dim), jnp.float32)
    carry = (start_max, start_total, start_accum)
    key_part = lax.all_gather(k_rot, "sp", axis=0, tiled=True)
    val_part = lax.all_gather(val_rows, "sp", axis=0, tiled=True)
    length = key_part.shape[0]
    factor = 4
    span = rows_here * factor
    turns = length // span
    key_blocks = key_part.reshape(turns, span, kv_here, head_dim)
    val_blocks = val_part.reshape(turns, span, kv_here, head_dim)
    carry, _ = lax.scan(key_block, carry, (key_blocks, val_blocks))
    maxima, totals, accum = carry
    attn = (
        jnp.transpose(accum / totals[..., None], (2, 0, 1, 3))
        .reshape(rows_here, heads_here * head_dim)
        .astype(jnp.bfloat16)
    )
    share = rows_here // lax.axis_size("tp")
    my_first = lax.axis_index("tp") * share
    proj = lax.psum_scatter(
        jnp.dot(attn, out_weight, preferred_element_type=jnp.float32).astype(jnp.bfloat16),
        "tp",
        scatter_dimension=0,
        tiled=True,
    ).astype(jnp.float32)
    my_resid = lax.dynamic_slice_in_dim(resid, my_first, share, 0)
    my_stream = (my_resid.astype(jnp.float32) + proj).astype(jnp.bfloat16)
    mixer_rows = lax.all_gather(normalize(my_stream, norm_gain), "tp", axis=0, tiled=True)

    def add_rows(shard_rows):
        return jnp.dot(mixer_rows, shard_rows, preferred_element_type=jnp.float32)

    gate = add_rows(lax.all_gather(gate_weight, "sp", axis=0, tiled=True))
    up_part = add_rows(lax.all_gather(up_weight, "sp", axis=0, tiled=True))
    hidden = (jax.nn.silu(gate) * up_part).astype(jnp.bfloat16)
    down_whole = lax.all_gather(down_weight, "sp", axis=1, tiled=True)
    down = lax.psum_scatter(
        jnp.dot(hidden, down_whole, preferred_element_type=jnp.float32).astype(jnp.bfloat16),
        "tp",
        scatter_dimension=0,
        tiled=True,
    ).astype(jnp.float32)
    return (my_stream.astype(jnp.float32) + 0.5 * down).astype(jnp.bfloat16)


SPLIT = 4


def fits(n_sp, kv_here, hidden_here):
    return n_sp % SPLIT == 0 and kv_here % SPLIT == 0 and hidden_here % (64 * SPLIT) == 0


def groups_of(n_sp):
    ranks = n_sp // SPLIT
    tokens = [[part * ranks + rank for part in range(SPLIT)] for rank in range(ranks)]
    hidden = [[part * ranks + rank for rank in range(ranks)] for part in range(SPLIT)]
    return tokens, hidden


MESH = pl.DeviceIdType.MESH


def layer_kernel(
    ranks,
    head_dim,
    key_ref,
    value_ref,
    query_ref,
    k_gain_ref,
    q_gain_ref,
    freq_ref,
    gate_ref,
    up_ref,
    down_ref,
    ow_ref,
    resid_ref,
    gain_ref,
    out_ref,
    kvb,
    qb,
    asend,
    ab,
    wgu,
    wdn,
    pj,
    prv,
    nb,
    st,
    dsb,
    drv,
    ds2,
    dzb,
    acc,
    kv_ref,
    q_ref,
    gu_ref,
    local_sem,
    kvz_s, kvz_r, kvx_s, kvx_r, q_s, q_r, gz_s, gz_r, dz_s, dz_r,
    gx_s, gx_r, dx_s, dx_r, gh_s, gh_r, dh_s, dh_r,
    at_s, at_r, pj_s, pj_r, nz_s, nz_r, np_s, np_r, dp_s, dp_r, fz_s, fz_r,
):
    sp = lax.axis_index("sp")
    core = lax.axis_index("tp")
    part = sp // ranks
    rank = sp % ranks
    rows = q_ref.shape[1]
    share = rows // 2
    depth = gu_ref.shape[1]
    width = down_ref.shape[0] // SPLIT
    cols = down_ref.shape[1]
    group = q_ref.shape[2] // head_dim
    other = 1 - core
    flips = (1, 2, 3)

    def flip(e):
        x = rank % 2
        y = rank // 2
        nx = 1 - x if e % 2 else x
        ny = 1 - y if e // 2 else y
        return ny * 2 + nx

    def peer_part(dz):
        return ((part + dz) % SPLIT) * ranks + rank

    def from_part(dz):
        return (part + SPLIT - dz) % SPLIT

    def near(e):
        return part * ranks + flip(e)

    def dn_own(index):
        return down_ref.at[pl.ds(pl.multiple_of(index * width, 16), width)]

    barrier = pltpu.get_barrier_semaphore()
    for dz in range(1, SPLIT):
        pl.semaphore_signal(barrier, inc=1, device_id=(peer_part(dz), core), device_id_type=MESH)
    for e in flips:
        pl.semaphore_signal(barrier, inc=1, device_id=(near(e), core), device_id_type=MESH)
    pl.semaphore_signal(barrier, inc=1, device_id=(sp, other), device_id_type=MESH)

    lane = lax.broadcasted_iota(jnp.int32, (rows, head_dim), 1)
    spot = sp * rows + lax.broadcasted_iota(jnp.int32, (rows, head_dim), 0)
    grid_bits = GRID_W.bit_length() - 1
    coords = jnp.where(lane < head_dim // 2, spot >> grid_bits, spot & (GRID_W - 1))
    angles = coords.astype(jnp.float32) * freq_ref[...]
    first_half = (lane & (head_dim // 2 - 1)) < head_dim // 4
    cosine = jnp.cos(angles)
    sine = jnp.where(first_half, -jnp.sin(angles), jnp.sin(angles))

    def turn(ref, head, gain):
        x = ref[:, head * head_dim : (head + 1) * head_dim].astype(jnp.float32)
        x = x * lax.rsqrt(jnp.mean(x * x, axis=-1, keepdims=True) + EPSILON) * gain[...]
        quarter = head_dim // 4
        mate = jnp.where(first_half, pltpu.roll(x, head_dim - quarter, 1), pltpu.roll(x, quarter, 1))
        return (x * cosine + mate * sine).astype(jnp.bfloat16)

    for index in range(SPLIT):
        kv_ref[index, :, 0:head_dim] = turn(key_ref, index, k_gain_ref)
        kv_ref[index, :, head_dim : 2 * head_dim] = value_ref[:, index * head_dim : (index + 1) * head_dim]
    for index in range(SPLIT):
        for head in range(group):
            lanes = slice(head * head_dim, (head + 1) * head_dim)
            q_ref[index, :, lanes] = turn(query_ref, index * group + head, q_gain_ref)
    whole_lanes = width // 128 * 128
    for index in range(SPLIT):
        start = index * width // 128 * 128
        skew = index * width - start
        rests = []
        for which, ref in enumerate((gate_ref, up_ref)):
            block = ref[:, start : start + whole_lanes + 128]
            if skew:
                block = pltpu.roll(block.astype(jnp.float32), whole_lanes + 128 - skew, 1).astype(jnp.bfloat16)
            gu_ref[index, :, which * whole_lanes : (which + 1) * whole_lanes] = block[:, :whole_lanes]
            rests.append(block[:, whole_lanes:].astype(jnp.float32))
        spread = lax.broadcasted_iota(jnp.int32, rests[0].shape, 1)
        last = jnp.where(spread < width - whole_lanes, rests[0], pltpu.roll(rests[1], width - whole_lanes, 1))
        gu_ref[index, :, 2 * whole_lanes :] = last.astype(jnp.bfloat16)

    sent = []

    def send(src, dst, s_sem, r_sem, target, keep=True):
        copy = pltpu.make_async_remote_copy(
            src_ref=src, dst_ref=dst, send_sem=s_sem, recv_sem=r_sem, device_id=target, device_id_type=MESH
        )
        copy.start()
        if keep:
            sent.append(copy)
        return copy

    def landed(dst, s_sem, r_sem):
        pltpu.make_async_remote_copy(
            src_ref=dst, dst_ref=dst, send_sem=s_sem, recv_sem=r_sem, device_id=(sp, other), device_id_type=MESH
        ).wait_recv()

    def gu_at(source, first=0, count=None):
        return wgu.at[pl.ds(pl.multiple_of(source * depth + first, 16), depth if count is None else count)]

    def dn_at(source, first=0, count=None):
        return wdn.at[pl.ds(first, width if count is None else count), pl.ds(pl.multiple_of(source * cols, cols), cols)]

    locals_ = [
        pltpu.make_async_copy(kv_ref.at[part], kvb.at[part, rank], local_sem.at[0]),
        pltpu.make_async_copy(q_ref.at[part], qb.at[part], local_sem.at[1]),
        pltpu.make_async_copy(gu_ref.at[part], gu_at(sp), local_sem.at[2]),
        pltpu.make_async_copy(dn_own(part), dn_at(sp), local_sem.at[3]),
    ]
    for copy in locals_:
        copy.start()
    pad = wdn.shape[0] - width
    wdn[pl.ds(width, pad), :] = jnp.zeros((pad, wdn.shape[1]), wdn.dtype)

    pl.semaphore_wait(barrier, SPLIT - 1 + 3 + 1)

    def to_part(dz):
        return (part + dz) % SPLIT

    for dz in range(1, SPLIT):
        send(kv_ref.at[to_part(dz)], kvb.at[part, rank], kvz_s.at[dz], kvz_r.at[dz], (peer_part(dz), core))
    for e in flips:
        send(kv_ref.at[part], kvb.at[part, rank], kvx_s.at[0, e], kvx_r.at[0, e], (near(e), core))
    for dz in range(1, SPLIT):
        send(q_ref.at[to_part(dz)], qb.at[part], q_s.at[dz], q_r.at[dz], (peer_part(dz), core))
    for e in (1, 2):
        send(dn_own(part), dn_at(sp), dx_s.at[0, e], dx_r.at[0, e], (near(e), core))
    for dz in range(1, SPLIT):
        send(gu_ref.at[to_part(dz)], gu_at(sp), gz_s.at[dz], gz_r.at[dz], (peer_part(dz), core))
        send(dn_own(to_part(dz)), dn_at(sp), dz_s.at[dz], dz_r.at[dz], (peer_part(dz), core))
    for dz in range(1, SPLIT):
        slot = kvb.at[from_part(dz), rank]
        landed(slot, kvz_s.at[dz], kvz_r.at[dz])
        for e in flips:
            send(slot, slot, kvx_s.at[dz, e], kvx_r.at[dz, e], (near(e), core))
    for e in (1, 2):
        send(gu_ref.at[part], gu_at(sp), gx_s.at[0, e], gx_r.at[0, e], (near(e), core))

    def pass_on(dz):
        source = from_part(dz) * ranks + rank
        landed(gu_at(source), gz_s.at[dz], gz_r.at[dz])
        for e in (1, 2):
            send(gu_at(source), gu_at(source), gx_s.at[dz, e], gx_r.at[dz, e], (near(e), core))
        landed(dn_at(source), dz_s.at[dz], dz_r.at[dz])
        for e in (1, 2):
            send(dn_at(source), dn_at(source), dx_s.at[dz, e], dx_r.at[dz, e], (near(e), core))

    def halves(dz):
        for e in (1, 2):
            source = from_part(dz) * ranks + flip(e)
            across = (near(3 - e), core)
            landed(gu_at(source), gx_s.at[dz, e], gx_r.at[dz, e])
            half = gu_at(source, (e - 1) * depth // 2, depth // 2)
            send(half, half, gh_s.at[dz, e], gh_r.at[dz, e], across)
            landed(dn_at(source), dx_s.at[dz, e], dx_r.at[dz, e])
            half = dn_at(source, (e - 1) * width // 2, width // 2)
            send(half, half, dh_s.at[dz, e], dh_r.at[dz, e], across)

    for dz in range(SPLIT):
        for e in flips:
            landed(kvb.at[from_part(dz), flip(e)], kvx_s.at[dz, e], kvx_r.at[dz, e])
    locals_[0].wait()
    locals_[1].wait()
    for dz in range(1, SPLIT):
        landed(qb.at[from_part(dz)], q_s.at[dz], q_r.at[dz])

    factor = head_dim ** (-0.5) * math.log2(math.e)
    length = SPLIT * ranks * rows

    def attend(source, target):
        @pl.loop(0, group)
        def _(head):
            lanes = pl.ds(pl.multiple_of(head * head_dim, head_dim), head_dim)
            q = qb[source, :, lanes]
            keys = kvb[:, :, :, pl.ds(0, head_dim)].reshape(length, head_dim)
            scores = lax.dot_general(q, keys, (((1,), (1,)), ((), ())), preferred_element_type=jnp.float32)
            peak = jnp.max(scores, axis=-1, keepdims=True)
            weights = jnp.exp2((scores - peak) * factor)
            total = jnp.sum(weights, axis=-1, keepdims=True)
            vals = kvb[:, :, :, pl.ds(head_dim, head_dim)].reshape(length, head_dim)
            summed = jnp.dot(weights.astype(jnp.bfloat16), vals, preferred_element_type=jnp.float32)
            target[:, lanes] = (summed / total).astype(jnp.bfloat16)

    for dz in (1, 2, 3):
        attend(to_part(dz), asend.at[dz])
        send(asend.at[dz], ab.at[part], at_s.at[dz], at_r.at[dz], (peer_part(dz), core))
        if dz == 2:
            pass_on(1)
    attend(part, ab.at[part])
    halves(0)
    for dz in range(1, SPLIT):
        landed(ab.at[from_part(dz)], at_s.at[dz], at_r.at[dz])

    attn = jnp.concatenate([ab[index] for index in range(SPLIT)], axis=1)
    tile = 512
    for first in range(0, ow_ref.shape[1], tile):
        block = jnp.dot(attn, ow_ref[:, first : first + tile], preferred_element_type=jnp.float32)
        pj[:, :, first : first + tile] = block.astype(jnp.bfloat16).reshape(2, share, tile)
    send(pj.at[other], prv, pj_s, pj_r, (sp, other))
    pass_on(2)
    landed(prv, pj_s, pj_r)
    proj = pj[core].astype(jnp.float32) + prv[...].astype(jnp.float32)
    stream = (resid_ref[pl.ds(pl.multiple_of(core * share, 16), share)].astype(jnp.float32) + proj).astype(jnp.bfloat16)
    st[...] = stream
    wide = stream.astype(jnp.float32)
    level = lax.rsqrt(jnp.mean(wide * wide, axis=-1, keepdims=True) + EPSILON)
    nb[part, core] = (wide * level * gain_ref[...]).astype(jnp.bfloat16)
    ahead = [(part < SPLIT - 1, sp + ranks, -1), (part > 0, sp - ranks, 1)]

    def step_on(source, step, way):
        slot = nb.at[source, core]
        go, target, _ = ahead[way]

        @pl.when(go)
        def _():
            send(slot, slot, nz_s.at[way, step], nz_r.at[way, step], (target, core), keep=False)

    def present(way, step):
        source = part + ahead[way][2] * (step + 1)
        return source, (source >= 0) & (source < SPLIT)

    step_on(part, 0, 0)
    step_on(part, 0, 1)
    mine = nb.at[part, core]
    send(mine, mine, np_s.at[part], np_r.at[part], (sp, other))
    def hop(step):
        for way in (0, 1):
            source, there = present(way, step)

            @pl.when(there)
            def _():
                slot = nb.at[source, core]
                landed(slot, nz_s.at[way, step], nz_r.at[way, step])
                if step < SPLIT - 2:
                    step_on(source, step + 1, way)
                send(slot, slot, np_s.at[source], np_r.at[source], (sp, other), keep=False)

    halves(1)
    pass_on(3)
    hop(0)
    halves(2)
    hop(1)
    halves(3)
    hop(2)
    for dz in range(SPLIT):
        for e in (1, 2):
            source = from_part(dz) * ranks + flip(3)
            landed(gu_at(source, (e - 1) * depth // 2, depth // 2), gh_s.at[dz, e], gh_r.at[dz, e])
            landed(dn_at(source, (e - 1) * width // 2, width // 2), dh_s.at[dz, e], dh_r.at[dz, e])
    locals_[2].wait()
    locals_[3].wait()

    main = width // 128 * 128
    half_lane = width - main

    def feed(source):
        landed(nb.at[source, other], np_s.at[source], np_r.at[source])
        x = nb[source].reshape(rows, nb.shape[-1])
        pieces = []
        gate = jnp.dot(x, wgu[:, pl.ds(0, main)], preferred_element_type=jnp.float32)
        up = jnp.dot(x, wgu[:, pl.ds(main, main)], preferred_element_type=jnp.float32)
        pieces.append((gate / (1.0 + jnp.exp(-gate)) * up).astype(jnp.bfloat16))
        last = jnp.dot(x, wgu[:, pl.ds(2 * main, 128)], preferred_element_type=jnp.float32)
        turned = pltpu.roll(last, half_lane, 1)
        lane = lax.broadcasted_iota(jnp.int32, last.shape, 1)
        tail = jnp.where(lane < half_lane, last / (1.0 + jnp.exp(-last)) * turned, 0.0)
        pieces.append(tail.astype(jnp.bfloat16))
        hidden = jnp.concatenate(pieces, axis=1)
        for first in range(0, wdn.shape[1], tile):
            block = jnp.dot(hidden, wdn[:, first : first + tile], preferred_element_type=jnp.float32)
            dsb[source, :, :, first : first + tile] = block.astype(jnp.bfloat16).reshape(2, share, tile)

    high, odd = part // 2, part % 2
    order = (3 - 3 * high, 2 - 2 * odd + high, 1 + odd, part)
    at_end = (part == 0) | (part == SPLIT - 1)
    inner = (part > 0) & (part < SPLIT - 1)

    def pair_sum(place):
        landed(drv.at[place], dp_s.at[place], dp_r.at[place])
        return dsb[order[place], core].astype(jnp.float32) + drv[place].astype(jnp.float32)

    def onward(place, first):
        target = order[place]
        way = 1 - (target > part).astype(jnp.int32)
        total = pair_sum(place)
        if not first:
            landed(dzb.at[way, target], fz_s.at[way, target], fz_r.at[way, target])
            total = total + dzb[way, target].astype(jnp.float32)
        ds2[target] = total.astype(jnp.bfloat16)
        slot = dzb.at[way, target]
        sender = fz_s.at[way, target]
        send(ds2.at[target], slot, sender, fz_r.at[way, target], (sp + ranks * (1 - 2 * way), core), keep=False)

    for place in range(SPLIT):
        feed(order[place])
        send(dsb.at[order[place], other], drv.at[place], dp_s.at[place], dp_r.at[place], (sp, other))
        if place:

            @pl.when(at_end)
            def _():
                onward(place - 1, True)

    @pl.when(inner)
    def _():
        for place in range(SPLIT - 1):
            onward(place, False)

    acc[...] = pair_sum(SPLIT - 1)
    for way, some in ((0, part > 0), (1, part < SPLIT - 1)):

        @pl.when(some)
        def _():
            landed(dzb.at[way, part], fz_s.at[way, part], fz_r.at[way, part])
            acc[...] += dzb[way, part].astype(jnp.float32)

    down = acc[...]
    out_ref[...] = (st[...].astype(jnp.float32) + 0.5 * down).astype(jnp.bfloat16)
    for copy in sent:
        copy.wait_send()

    def left(src, s_sem, r_sem):
        pltpu.make_async_remote_copy(
            src_ref=src, dst_ref=src, send_sem=s_sem, recv_sem=r_sem, device_id=(sp, other), device_id_type=MESH
        ).wait_send()

    for way in (0, 1):
        for step in range(SPLIT - 1):
            source, there = present(way, step)

            @pl.when(there)
            def _():
                left(nb.at[source, core], np_s.at[source], np_r.at[source])

        for step in range(SPLIT - 1):
            source = part + ahead[way][2] * step

            @pl.when(ahead[way][0] & (source >= 0) & (source < SPLIT))
            def _():
                left(nb.at[source, core], nz_s.at[way, step], nz_r.at[way, step])

    for place in range(SPLIT - 1):
        target = order[place]
        way = 1 - (target > part).astype(jnp.int32)
        left(ds2.at[target], fz_s.at[way, target], fz_r.at[way, target])


def run_layer(key, value, query, k_gain, q_gain, gate, up, down, out_weight, resid, gain, ranks):
    rows = query.shape[0]
    share = rows // 2
    model = resid.shape[1]
    width = down.shape[0] // SPLIT
    depth = gate.shape[0]
    head_dim = q_gain.shape[0]
    n_sp = ranks * SPLIT
    quarter = head_dim // 4
    steps = np.tile(np.arange(quarter, dtype=np.float32), 4)
    freq = jnp.asarray((np.float64(10000.0) ** (-steps / quarter)).astype(np.float32))[None, :]
    half = jnp.bfloat16
    dma = pltpu.SemaphoreType.DMA
    per_part = [dma((SPLIT,))] * 2
    per_near = [dma((SPLIT, 4))] * 2
    per_way = [dma((2, SPLIT))] * 2
    anywhere = pl.BlockSpec(memory_space=pl.ANY)
    inside = pl.BlockSpec(memory_space=pltpu.VMEM)
    kv_shape = (SPLIT, rows, 2 * head_dim)
    q_shape = (SPLIT, rows, query.shape[1] // SPLIT)
    return pl.pallas_call(
        functools.partial(layer_kernel, ranks, head_dim),
        out_shape=jax.ShapeDtypeStruct((share, model), half),
        in_specs=[inside] * 8 + [anywhere] + [inside] * 3,
        out_specs=inside,
        scratch_shapes=[
            pltpu.VMEM((SPLIT, ranks, rows, 2 * head_dim), half),
            pltpu.VMEM(q_shape, half),
            pltpu.VMEM(q_shape, half),
            pltpu.VMEM(q_shape, half),
            pltpu.VMEM((n_sp * depth, 2 * width), half),
            pltpu.VMEM((-(-width // 128) * 128, model), half),
            pltpu.VMEM((2, share, model), half),
            pltpu.VMEM((share, model), half),
            pltpu.VMEM((SPLIT, 2, share, model), half),
            pltpu.VMEM((share, model), half),
            pltpu.VMEM((SPLIT, 2, share, model), half),
            pltpu.VMEM((SPLIT, share, model), half),
            pltpu.VMEM((SPLIT, share, model), half),
            pltpu.VMEM((2, SPLIT, share, model), half),
            pltpu.VMEM((share, model), jnp.float32),
            pltpu.VMEM(kv_shape, half),
            pltpu.VMEM(q_shape, half),
            pltpu.VMEM((SPLIT, depth, 2 * width), half),
            dma((4,)),
        ]
        + per_part + per_near + per_part * 3
        + per_near * 4
        + per_part + [dma, dma] + per_way + per_part * 2 + per_way,
        compiler_params=pltpu.CompilerParams(
            collective_id=0, has_side_effects=True, vmem_limit_bytes=62 * 1024 * 1024
        ),
    )(
        key, value, query, k_gain[None, :], q_gain[None, :], freq, gate, up, down, out_weight, resid, gain[None, :]
    )


def in_kernel(n_sp, n_tp, kv_here, head_dim, width):
    return n_sp == 4 * SPLIT and n_tp == 2 and kv_here == SPLIT and head_dim == 128 and width % 128 == 64


def body(
    resid,
    query,
    key,
    value,
    q_gain,
    k_gain,
    out_weight,
    norm_gain,
    gate_weight,
    up_weight,
    down_weight,
):
    rows = query.shape[0]
    head_dim = q_gain.shape[0]
    heads_here = query.shape[1] // head_dim
    kv_here = key.shape[1] // head_dim
    n_sp = lax.axis_size("sp")
    if not fits(n_sp, kv_here, gate_weight.shape[1]):
        return whole_body(
            resid, query, key, value, q_gain, k_gain, out_weight, norm_gain, gate_weight, up_weight, down_weight
        )
    hidden_part = gate_weight.shape[1] // SPLIT
    ranks = n_sp // SPLIT
    if in_kernel(n_sp, lax.axis_size("tp"), kv_here, head_dim, hidden_part):
        return run_layer(
            key, value, query, k_gain, q_gain, gate_weight, up_weight, down_weight, out_weight, resid, norm_gain, ranks
        )
    tok_groups, hid_groups = groups_of(n_sp)
    ranks = n_sp // SPLIT
    group_size = heads_here // kv_here
    kv_part = kv_here // SPLIT

    def swap(array):
        return lax.all_to_all(array, "sp", 0, 0, axis_index_groups=tok_groups, tiled=True)

    def spread(array, axis):
        return lax.all_gather(array, "sp", axis=axis, axis_index_groups=hid_groups, tiled=True)

    positions = lax.axis_index("sp") * rows + jnp.arange(rows, dtype=jnp.int32)
    q_rot = prepare(query.reshape(rows, heads_here, head_dim), q_gain, positions)
    k_rot = prepare(key.reshape(rows, kv_here, head_dim), k_gain, positions)
    cut = lambda a: a.reshape(a.shape[0], SPLIT, -1).transpose(1, 0, 2).reshape(SPLIT * a.shape[0], -1)
    k_rot, val = cut(k_rot), cut(value)
    pair = swap(jnp.concatenate([k_rot, val], axis=1))
    pair = spread(pair, 0)
    q_mine = swap(cut(q_rot))
    width = kv_part * head_dim
    keys = pair[:, :width].reshape(-1, kv_part, head_dim)
    vals = pair[:, width:].reshape(-1, kv_part, head_dim)
    grouped = q_mine.reshape(SPLIT * rows, kv_part, group_size, head_dim)
    gate_up = spread(swap(jnp.concatenate([cut(gate_weight), cut(up_weight)], axis=1)), 0)
    depth = gate_weight.shape[0]
    gate_up = gate_up.reshape(ranks, SPLIT, depth, -1).transpose(1, 0, 2, 3).reshape(n_sp * depth, -1)
    down_w = swap(down_weight)
    part = down_weight.shape[0] // SPLIT
    down_w = down_w.reshape(SPLIT, part, -1)
    down_w = lax.all_gather(down_w, "sp", axis=1, axis_index_groups=hid_groups)
    down_w = jnp.transpose(down_w, (2, 0, 1, 3)).reshape(part, -1)
    scores = jnp.einsum("qkgd,skd->kgqs", grouped, keys, preferred_element_type=jnp.float32) * head_dim ** (-0.5)
    weights = jnp.exp(scores - jnp.max(scores, axis=-1, keepdims=True))
    totals = jnp.sum(weights, axis=-1)
    accum = jnp.einsum("kgqs,skd->kgqd", weights.astype(jnp.bfloat16), vals, preferred_element_type=jnp.float32)
    attn = jnp.transpose(accum / totals[..., None], (2, 0, 1, 3)).astype(jnp.bfloat16).reshape(SPLIT * rows, -1)
    attn = swap(attn).reshape(SPLIT, rows, -1).transpose(1, 0, 2).reshape(rows, -1)
    return finish(attn, resid, out_weight, norm_gain, gate_up, down_w, tok_groups)


def finish(attn, resid, out_weight, norm_gain, gate_up, down_w, tok_groups):
    rows = resid.shape[0]
    n_tp = lax.axis_size("tp")
    share = rows // n_tp
    my_first = lax.axis_index("tp") * share
    proj = lax.psum_scatter(
        jnp.dot(attn, out_weight, preferred_element_type=jnp.float32).astype(jnp.bfloat16),
        "tp",
        scatter_dimension=0,
        tiled=True,
    ).astype(jnp.float32)
    my_resid = lax.dynamic_slice_in_dim(resid, my_first, share, 0)
    my_stream = (my_resid.astype(jnp.float32) + proj).astype(jnp.bfloat16)
    normed = normalize(my_stream, norm_gain)
    normed = lax.all_gather(normed, "sp", axis=0, axis_index_groups=tok_groups, tiled=False)
    normed = lax.all_gather(normed, "tp", axis=0, tiled=False)
    normed = normed.reshape(n_tp * SPLIT * share, -1)
    both = jnp.dot(normed, gate_up, preferred_element_type=jnp.float32)
    gate, up_part = jnp.split(both, 2, axis=1)
    hidden = (jax.nn.silu(gate) * up_part).astype(jnp.bfloat16)
    down = jnp.dot(hidden, down_w, preferred_element_type=jnp.float32).astype(jnp.bfloat16)
    down = lax.psum_scatter(down, "tp", scatter_dimension=0, tiled=True)
    down = lax.all_to_all(
        down.reshape(SPLIT, share, -1), "sp", 0, 0, axis_index_groups=tok_groups, tiled=True
    )
    down = jnp.sum(down.astype(jnp.float32), axis=0)
    return (my_stream.astype(jnp.float32) + 0.5 * down).astype(jnp.bfloat16)


def solution(mesh):
    placed = (
        P("sp", None),
        P("sp", "tp"),
        P("sp", "tp"),
        P("sp", "tp"),
        P(),
        P(),
        P("tp", None),
        P(),
        P("sp", "tp"),
        P("sp", "tp"),
        P("tp", "sp"),
    )
    return jax.shard_map(
        body, mesh=mesh, in_specs=placed, out_specs=P(("sp", "tp"), None), check_vma=False
    )
```
